512 devices in a mesh: ep: 128 (over z, y, core), tp: 4 (over x).
Axes of the slice: x: 4, y: 8, z: 8, core: 2. Of those that a mesh axis runs over, the one named last changes fastest.
Arguments:
- tokens: bfloat16 [2048, 1024], P(('ep', 'tp')), may hold values from -6 to 6
- lengths: int32 [2048], P(('ep', 'tp')), may hold values from 256 to 1024, as said below
- cache_latent: bfloat16 [2048, 1024, 256], P(('ep', 'tp')), may hold values from -160 to 160
- cache_rope: bfloat16 [2048, 32, 1024], P(('ep', 'tp')), may hold values from -6 to 6
- attn_gain: float32 [1024], replicated, may hold values from 0.1 to 1.9
- latent_gain: float32 [256], replicated, may hold values from 0.1 to 1.9
- post_gain: float32 [1024], replicated, may hold values from 0.1 to 1.9
- ffn_gain: float32 [1024], replicated, may hold values from 0.1 to 1.9
- out_gain: float32 [1024], replicated, may hold values from 0.1 to 1.9
- w_latent: bfloat16 [1024, 256], P(None, 'tp'), may hold values from -0.1875 to 0.1875
- w_rope_key: bfloat16 [1024, 32], replicated, may hold values from -0.1875 to 0.1875
- w_query: bfloat16 [1024, 768], P(None, 'tp'), may hold values from -0.1875 to 0.1875
- w_absorb_key: bfloat16 [8, 64, 256], P('tp'), may hold values from -0.75 to 0.75
- w_absorb_value: bfloat16 [8, 256, 64], P('tp'), may hold values from -0.375 to 0.375
- w_out: bfloat16 [512, 1024], P('tp'), may hold values from -0.25 to 0.25
- routes: int32 [2048, 6], P(('ep', 'tp')), may hold values from 0 to 127, all different within a row; in each aligned block of 16 rows (0 to 15, 16 to 31, ...) at most 2 rows name the same one
- route_weights: float32 [2048, 6], P(('ep', 'tp')), may hold values from 0.2 to 1
- w_exp_gate: bfloat16 [128, 1024, 256], P('ep'), may hold values from -0.1875 to 0.1875
- w_exp_up: bfloat16 [128, 1024, 256], P('ep'), may hold values from -0.1875 to 0.1875
- w_exp_down: bfloat16 [128, 256, 1024], P('ep'), may hold values from -0.375 to 0.375
- w_dense_gate: bfloat16 [4096, 1024], P('ep'), may hold values from -0.1875 to 0.1875
- w_dense_up: bfloat16 [4096, 1024], P('ep'), may hold values from -0.1875 to 0.1875
- w_dense_down: bfloat16 [4096, 1024], P('ep'), may hold values from -0.09375 to 0.09375
- dense_gate_vector: float32 [1024], replicated, may hold values from -0.1875 to 0.1875
Outputs:
- output: bfloat16 [2048, 1024], P(('ep', 'tp'))
- new_latent: bfloat16 [2048, 256], P(('ep', 'tp'))
- new_rope_key: bfloat16 [2048, 32], P(('ep', 'tp'))
The draws below stay inside these ranges and needn't reach their ends.
Inputs may be any that keep to these rules, and one draw needn't show every extreme that they name: `routes`: in each aligned block of 16 rows no expert is named by more than 2 rows; each row names 6 different experts. `lengths`: some sequence holds exactly 1024 cached positions.
All inputs are finite; a program needn't handle non-finite values.
Results may differ from the reference program's by a relative error of at most 0.015.
Values may be sent and summed in bfloat16 or wider, within the bound.
A program may use at most 64 MiB of HBM per device.

```python
import math
import jax
import jax.numpy as jnp
import numpy as np
from jax import lax

D = 1024
HEADS = 8
NOPE = 64
ROPE = 32
V_HEAD = 64
KV_RANK = 256
EXPERT_FF = 256
SH_FF = 4096
TOPK = 6
CACHE_LEN = 1024
SEQ_GRP = 16
BATCH = 2048
EXPERTS = 128
CAP = 2
N_EP = 128
N_TP = 4


def draw_lengths(key, part):
    first_key, second_key = jax.random.split(key)
    drawn = jax.random.randint(first_key, (BATCH,), CACHE_LEN // 4, CACHE_LEN + 1)
    chosen = jax.random.randint(second_key, (), 0, BATCH)
    return jnp.where(jnp.arange(BATCH) == chosen, CACHE_LEN, drawn).astype(jnp.int32)


def draw_cache_latent(key, part):
    keys = jax.random.split(key, 1)
    base = jnp.clip(jax.random.normal(keys[0], (BATCH, CACHE_LEN, KV_RANK), jnp.float32), -4.0, 4.0)
    return base.astype(jnp.bfloat16)


def block_levels(rng, shape, cuts, smallest, largest):
    def one(dim, blocks):
        draws = jax.random.uniform(jax.random.fold_in(jax.random.fold_in(rng, 6), dim), (blocks,), jnp.float32, smallest / len(cuts), largest / len(cuts))
        return jnp.repeat(jnp.exp(draws), shape[dim] // blocks).reshape((-1,) + (1,) * (len(shape) - dim - 1))

    level = one(*cuts[0])
    for cut in cuts[1:]:
        level = level * one(*cut)
    return level


def deal_out(key, own, number, rows, number_of, top, bound, skew):
    ranking = jax.random.permutation(key, number_of)
    packed, ordinary = load_shares(number_of, rows * top, bound, skew, True), load_shares(number_of, rows * top, bound, skew, False)
    places = jnp.arange(number_of)

    def named(sizes, rotation):
        used = int((sizes > 0).sum())
        fixed = max(1, used // 4)
        shifted = fixed + (places - fixed + rotation * (used - fixed)) % max(1, number_of - fixed)
        return jnp.zeros((number_of,), jnp.int32).at[ranking[jnp.where(places < fixed, places, shifted)]].set(jnp.asarray(sizes, jnp.int32))

    sizes = jnp.where(number % 4 == 0, named(packed, number // 4), named(ordinary, number - number // 4 - 1))
    mixed = jax.random.permutation(jax.random.fold_in(own, 3), number_of)
    source_of, sink = mixed[0:number_of // 2 * 2:2], mixed[1:number_of // 2 * 2:2]
    margin = jnp.minimum(sizes[source_of] - 1, bound - sizes[sink]) // 2
    margin = jnp.where((source_of == ranking[0]) | (sink == ranking[0]) | (sizes[sink] == 0), 0, jnp.maximum(margin, 0))
    shifted = jax.random.randint(jax.random.fold_in(own, 4), (number_of // 2,), 0, 1 << 20) % (margin + 1)
    sizes = sizes.at[source_of].add(-shifted).at[sink].add(shifted)
    items = jnp.searchsorted(jnp.cumsum(sizes), jnp.arange(rows * top), side="right").astype(jnp.int32)
    grid = items.reshape(top, rows).T
    grid = grid[jax.random.permutation(jax.random.fold_in(own, 1), rows)]
    rotation = jax.random.randint(jax.random.fold_in(own, 2), (rows, 1), 0, top)
    return jnp.take_along_axis(grid, (jnp.arange(top)[None, :] + rotation) % top, axis=1)


def load_shares(number_of, total, bound, lean, full):
    weights = [(1 << 20) // math.isqrt(standing ** lean) + 1 for standing in range(1, number_of + 1)]
    largest = bound if full else min(bound, max(-(-total // number_of), total * weights[0] // sum(weights)))
    least = 1 if total - largest >= number_of - 1 else 0
    holding, spare = [largest] + [least] * (number_of - 1), total - largest - least * (number_of - 1)
    while spare > 0:
        candidates = [i for i in range(1, number_of) if holding[i] < largest] or [i for i in range(1, number_of) if holding[i] < bound]
        whole, budget = sum([weights[i] for i in candidates]), spare
        for i in candidates:
            extra = min(bound - holding[i], max(1, budget * weights[i] // whole), spare)
            holding[i] = holding[i] + extra
            spare = spare - extra
    return np.array(holding)


def gaussian(stream_key, extent, scale, limit, cuts=(), kind=jnp.bfloat16):
    values = jax.random.normal(stream_key, extent, jnp.float32) * scale
    if len(cuts) > 0:
        values = block_levels(stream_key, extent, cuts, -0.22, 0.18) * values
    return jnp.clip(values, min=-limit, max=limit).astype(kind)


def setup_inputs(seed: int = 0) -> dict:
    arg_keys = jax.random.split(jax.random.key(seed), 25)
    tokens = gaussian(arg_keys[0], (BATCH, D), 1.0, 6.0, ((0, 512),))
    lengths = draw_lengths(jax.random.fold_in(arg_keys[24], 71), 0)
    cache_latent = draw_cache_latent(jax.random.fold_in(arg_keys[24], 71), 0)
    cache_rope = gaussian(arg_keys[3], (BATCH, ROPE, CACHE_LEN), 1.0, 6.0, ((0, 512),))
    attn_gain = jnp.clip(1.0 + 0.18 * jax.random.normal(arg_keys[4], (D,), jnp.float32), 0.1, 1.9)
    latent_gain = jnp.clip(1.0 + 0.18 * jax.random.normal(arg_keys[5], (KV_RANK,), jnp.float32), 0.1, 1.9)
    post_gain = jnp.clip(1.0 + 0.18 * jax.random.normal(arg_keys[6], (D,), jnp.float32), 0.1, 1.9)
    ffn_gain = jnp.clip(1.0 + 0.18 * jax.random.normal(arg_keys[7], (D,), jnp.float32), 0.1, 1.9)
    out_gain = jnp.clip(1.0 + 0.18 * jax.random.normal(arg_keys[8], (D,), jnp.float32), 0.1, 1.9)
    w_latent = gaussian(arg_keys[9], (D, KV_RANK), D ** -0.5, 0.1875, ((1, 4),))
    w_rope_key = gaussian(arg_keys[10], (D, ROPE), D ** -0.5, 0.1875)
    w_query = gaussian(arg_keys[11], (D, HEADS * (NOPE + ROPE)), D ** -0.5, 0.1875, ((1, 4),))
    w_absorb_key = gaussian(arg_keys[12], (HEADS, NOPE, KV_RANK), NOPE ** -0.5, 0.75, ((0, 4),))
    w_absorb_value = gaussian(arg_keys[13], (HEADS, KV_RANK, V_HEAD), KV_RANK ** -0.5, 0.375, ((0, 4),))
    w_out = gaussian(arg_keys[14], (HEADS * V_HEAD, D), (HEADS * V_HEAD) ** -0.5, 0.25, ((0, 4),))
    routes_keys = jax.random.split(jax.random.fold_in(arg_keys[15], 1), BATCH // SEQ_GRP)
    routes_turns = jax.random.permutation(jax.random.fold_in(arg_keys[15], 3), BATCH // SEQ_GRP)
    routes = jax.vmap(lambda own, number: deal_out(jax.random.fold_in(arg_keys[15], 2), own, number, SEQ_GRP, EXPERTS, TOPK, CAP, 2))(routes_keys, routes_turns).reshape((BATCH, TOPK))
    route_weights = jnp.clip(0.2 + 0.8 * jax.random.uniform(arg_keys[16], (BATCH, TOPK), jnp.float32) ** block_levels(arg_keys[16], (BATCH, TOPK), ((0, 512),), -0.2, 0.2), 0.2, 1.0)
    w_exp_gate = gaussian(arg_keys[17], (EXPERTS, D, EXPERT_FF), D ** -0.5, 0.1875, ((0, 128),))
    w_exp_up = gaussian(arg_keys[18], (EXPERTS, D, EXPERT_FF), D ** -0.5, 0.1875, ((0, 128),))
    w_exp_down = gaussian(arg_keys[19], (EXPERTS, EXPERT_FF, D), EXPERT_FF ** -0.5, 0.375, ((0, 128),))
    w_dense_gate = gaussian(arg_keys[20], (SH_FF, D), D ** -0.5, 0.1875, ((0, 128),))
    w_dense_up = gaussian(arg_keys[21], (SH_FF, D), D ** -0.5, 0.1875, ((0, 128),))
    w_dense_down = gaussian(arg_keys[22], (SH_FF, D), SH_FF ** -0.5, 0.09375, ((0, 128),))
    dense_gate_vector = gaussian(arg_keys[23], (D,), D ** -0.5, 0.1875, (), jnp.float32)
    return {"tokens": tokens, "lengths": lengths, "cache_latent": cache_latent, "cache_rope": cache_rope, "attn_gain": attn_gain, "latent_gain": latent_gain, "post_gain": post_gain, "ffn_gain": ffn_gain, "out_gain": out_gain, "w_latent": w_latent, "w_rope_key": w_rope_key, "w_query": w_query, "w_absorb_key": w_absorb_key, "w_absorb_value": w_absorb_value, "w_out": w_out, "routes": routes, "route_weights": route_weights, "w_exp_gate": w_exp_gate, "w_exp_up": w_exp_up, "w_exp_down": w_exp_down, "w_dense_gate": w_dense_gate, "w_dense_up": w_dense_up, "w_dense_down": w_dense_down, "dense_gate_vector": dense_gate_vector}


epsilon = 1e-06
rope_base = 10000.0
negative = -1e+30

def normalize(values, gain_vec):
    values = values.astype(jnp.float32)
    return values * lax.rsqrt(lax.optimization_barrier(jnp.mean(values * values, axis=-1, keepdims=True)) + epsilon) * gain_vec

def rotate(values, positions):
    half_width = values.shape[-1] // 2
    inverse = rope_base ** (-jnp.arange(half_width, dtype=jnp.float32) / half_width)
    angles = positions.astype(jnp.float32)[..., None] * inverse
    cosine = jnp.cos(angles)
    sine_part = jnp.sin(angles)
    first_half = values[..., :half_width]
    second = values[..., half_width:]
    return jnp.concatenate([first_half * cosine - second * sine_part, first_half * sine_part + second * cosine], axis=-1)

def attend(operands):
    q_latent, q_rope, cache_lat, cache_rot, new_lat, new_rot, seq_lengths = operands
    scaling = (NOPE + ROPE) ** (-0.5)
    scores = jnp.einsum('shc,slc->shl', q_latent.astype(jnp.float32), cache_lat.astype(jnp.float32))
    scores = scores + jnp.einsum('shr,srl->shl', q_rope.astype(jnp.float32), cache_rot.astype(jnp.float32))
    scores = scores * scaling
    own_score = lax.optimization_barrier(jnp.sum(q_latent.astype(jnp.float32) * new_lat.astype(jnp.float32)[:, None, :], axis=-1))
    own_score = (own_score + lax.optimization_barrier(jnp.sum(q_rope.astype(jnp.float32) * new_rot.astype(jnp.float32)[:, None, :], axis=-1))) * scaling
    visible = jnp.arange(cache_lat.shape[1], dtype=jnp.int32)[None, None, :] < seq_lengths[:, None, None]
    scores = jnp.where(visible, scores, negative)
    row_max = jnp.maximum(lax.optimization_barrier(jnp.max(scores, axis=-1)), own_score)
    weights = jnp.exp(scores - row_max[..., None])
    own_weight = jnp.exp(own_score - row_max)
    totals = lax.optimization_barrier(jnp.sum(weights, axis=-1)) + own_weight
    probabilities = (weights / totals[..., None]).astype(jnp.bfloat16)
    own_prob = (own_weight / totals).astype(jnp.bfloat16)
    mixed = jnp.einsum('shl,slc->shc', probabilities.astype(jnp.float32), cache_lat.astype(jnp.float32))
    mixed = mixed + own_prob.astype(jnp.float32)[..., None] * new_lat.astype(jnp.float32)[:, None, :]
    return mixed.astype(jnp.bfloat16)

def reference(tokens, lengths, cache_latent, cache_rope, attn_gain, latent_gain, post_gain, ffn_gain, out_gain, w_latent, w_rope_key, w_query, w_absorb_key, w_absorb_value, w_out, routes, route_weights, w_exp_gate, w_exp_up, w_exp_down, w_dense_gate, w_dense_up, w_dense_down, dense_gate_vector):
    hidden = normalize(tokens, attn_gain).astype(jnp.bfloat16)
    new_latent = normalize(jnp.dot(hidden, w_latent, preferred_element_type=jnp.float32), latent_gain).astype(jnp.bfloat16)
    new_rope_key = rotate(jnp.dot(hidden, w_rope_key, preferred_element_type=jnp.float32), lengths).astype(jnp.bfloat16)
    queries = jnp.dot(hidden, w_query, preferred_element_type=jnp.float32).astype(jnp.bfloat16)
    queries = queries.reshape(BATCH, HEADS, NOPE + ROPE)
    query_rope = rotate(queries[..., NOPE:].astype(jnp.float32), lengths[:, None]).astype(jnp.bfloat16)
    query_latent = jnp.einsum('shn,hnc->shc', queries[..., :NOPE].astype(jnp.float32), w_absorb_key.astype(jnp.float32)).astype(jnp.bfloat16)

    def grouped(array):
        return array.reshape((N_EP, SEQ_GRP) + array.shape[1:])
    attended = lax.map(attend, (grouped(query_latent), grouped(query_rope), grouped(cache_latent), grouped(cache_rope), grouped(new_latent), grouped(new_rope_key), grouped(lengths)))
    attended = attended.reshape(BATCH, HEADS, KV_RANK)
    head_out = jnp.einsum('shc,hcv->shv', attended.astype(jnp.float32), w_absorb_value.astype(jnp.float32)).astype(jnp.bfloat16)
    per_group = HEADS // N_TP
    pieces = jnp.einsum('sgk,gkd->sgd', head_out.reshape(BATCH, N_TP, per_group * V_HEAD).astype(jnp.float32), w_out.reshape(N_TP, per_group * V_HEAD, D).astype(jnp.float32))
    pieces = lax.optimization_barrier(pieces.astype(jnp.bfloat16))
    mixed = lax.optimization_barrier(jnp.sum(pieces.astype(jnp.float32), axis=1))
    residual = (tokens.astype(jnp.float32) + normalize(mixed, post_gain)).astype(jnp.bfloat16)
    ffn_in = normalize(residual, ffn_gain).astype(jnp.bfloat16)
    flattened = routes.reshape(N_EP, SEQ_GRP * TOPK)
    onehot = (flattened[..., None] == jnp.arange(EXPERTS, dtype=jnp.int32)).astype(jnp.int32)
    order_rank = lax.optimization_barrier(jnp.sum((jnp.cumsum(onehot, axis=1) - onehot) * onehot, axis=-1))
    slot_index = flattened * (N_EP * CAP) + jnp.arange(N_EP, dtype=jnp.int32)[:, None] * CAP + order_rank
    slot_index = slot_index.reshape(-1).astype(jnp.int32)
    repeated = jnp.repeat(ffn_in, TOPK, axis=0)
    buffer = jnp.zeros((EXPERTS * N_EP * CAP, D), jnp.bfloat16).at[slot_index].set(repeated)
    buffer = buffer.reshape(EXPERTS, N_EP * CAP, D)

    def expert(operands):
        rows_in, gate_w, up_w, down_w = operands
        gate_pre = jnp.dot(rows_in, gate_w, preferred_element_type=jnp.float32)
        up_proj = jnp.dot(rows_in, up_w, preferred_element_type=jnp.float32)
        activity = (jax.nn.silu(gate_pre) * up_proj).astype(jnp.bfloat16)
        return jnp.dot(activity, down_w, preferred_element_type=jnp.float32).astype(jnp.bfloat16)
    results = lax.map(expert, (buffer, w_exp_gate, w_exp_up, w_exp_down)).reshape(EXPERTS * N_EP * CAP, D)
    picked = results[slot_index.reshape(BATCH, TOPK)]
    routed = lax.optimization_barrier(jnp.sum(route_weights[..., None] * picked.astype(jnp.float32), axis=1))
    dense_pre = jnp.dot(ffn_in, w_dense_gate.T, preferred_element_type=jnp.float32)
    dense_up = jnp.dot(ffn_in, w_dense_up.T, preferred_element_type=jnp.float32)
    dense_act = (jax.nn.silu(dense_pre) * dense_up).astype(jnp.bfloat16)
    dense_out = jnp.dot(dense_act, w_dense_down, preferred_element_type=jnp.float32)
    dense_gate = jax.nn.sigmoid(lax.optimization_barrier(jnp.sum(ffn_in.astype(jnp.float32) * dense_gate_vector, axis=-1)))
    combined = routed + dense_gate[:, None] * dense_out
    output = (residual.astype(jnp.float32) + normalize(combined, out_gain)).astype(jnp.bfloat16)
    return (output, new_latent, new_rope_key)
```

```python
import functools

import jax
import jax.numpy as jnp
from jax import lax
from jax.experimental import pallas as pl
from jax.experimental.pallas import tpu as pltpu
from jax.sharding import Mesh
from jax.sharding import PartitionSpec as P

EP = ("ep_0", "ep_1", "ep_2")
EP_TP = ("ep_0", "ep_1", "ep_2", "tp")
MESH = pl.DeviceIdType.MESH
F32 = jnp.float32
BF16 = jnp.bfloat16

epsilon = 1e-06
rope_base = 10000.0
negative = -1e30


def dot(a, b):
    return jnp.dot(a, b, preferred_element_type=F32)


def dot_nt(a, b):
    return lax.dot_general(a, b, (((1,), (1,)), ((), ())), preferred_element_type=F32)


def normalize(values, gain):
    values = values.astype(F32)
    mean = jnp.mean(values * values, axis=-1, keepdims=True)
    return values * lax.rsqrt(mean + epsilon) * gain


def swap_halves(values):
    half = values.shape[-1] // 2
    return jnp.concatenate([values[:, half:], values[:, :half]], axis=1)


def silu(values):
    return values / (1.0 + jnp.exp(-values))


def exchange(axis, size, me, src_of, dst, send, recv):
    copies = []
    for k in range(1, size):
        partner = lax.rem(me + k, size)
        copy = pltpu.make_async_remote_copy(
            src_ref=src_of(partner),
            dst_ref=dst.at[me],
            send_sem=send.at[k - 1],
            recv_sem=recv.at[me],
            device_id={axis: partner},
            device_id_type=MESH,
        )
        copy.start()
        copies.append(copy)
    return copies


def arrived(axis, size, me, dst, send, recv):
    for k in range(1, size):
        partner = lax.rem(me + k, size)
        pltpu.make_async_remote_copy(
            src_ref=dst.at[partner],
            dst_ref=dst.at[partner],
            send_sem=send.at[k - 1],
            recv_sem=recv.at[partner],
            device_id={axis: partner},
            device_id_type=MESH,
        ).wait_recv()


def greet(axes):
    barrier = pltpu.get_barrier_semaphore()
    total = 0
    for axis, size in axes:
        me = lax.axis_index(axis)
        for k in range(1, size):
            pl.semaphore_signal(
                barrier,
                inc=1,
                device_id={axis: lax.rem(me + k, size)},
                device_id_type=MESH,
            )
            total += 1
    pl.semaphore_wait(barrier, total)


def attention_kernel(
    sizes,
    lengths, tokens, cosines, sines, attn_gain, latent_gain, post_gain, ffn_gain,
    w_latent, w_rope_key, w_query, w_absorb_key, w_absorb_value, w_out,
    cache_latent, cache_rope,
    residual_out, ffn_out, latent_out, rope_out,
    lat, rop, hid, stack, qmsg_src, qmsg, fmsg_src, fmsg, wk_pad, q_lat, q_rot,
    att_src_f, att_src, att, att_stack, mix_src, mix,
    cache_sem, hid_send, hid_recv, q_send, q_recv, f_send, f_recv,
    att_send, att_recv, mix_send, mix_recv,
):
    nx = sizes["tp"]
    rows = tokens.shape[0]
    x = lax.axis_index("tp")
    lat_copy = pltpu.make_async_copy(cache_latent, lat, cache_sem.at[0])
    rop_copy = pltpu.make_async_copy(cache_rope, rop, cache_sem.at[1])
    lat_copy.start()
    rop_copy.start()
    greet((("tp", nx),))

    toks = tokens[...].astype(F32)
    hidden = normalize(toks, attn_gain[...]).astype(BF16)
    hid[x] = hidden
    hid_copies = exchange("tp", nx, x, lambda p: hid.at[x], hid, hid_send, hid_recv)
    cos = cosines[...]
    sin = sines[...]
    rope_pre = dot(hidden, w_rope_key[...])
    new_rope = (rope_pre * cos + swap_halves(rope_pre) * sin).astype(BF16)
    rope_out[...] = new_rope
    heads = w_absorb_key.shape[0]
    nope = w_absorb_key.shape[1]
    rank = w_absorb_key.shape[2]
    span = w_query.shape[1] // heads
    rope = span - nope
    wk_pad[...] = jnp.zeros(wk_pad.shape, BF16)
    for h in range(heads):
        wk_pad[h * span : h * span + nope, h * rank : (h + 1) * rank] = w_absorb_key[h]
    arrived("tp", nx, x, hid, hid_send, hid_recv)
    for t in range(nx):
        stack[t * rows : (t + 1) * rows, :] = hid[t].astype(F32)
    group_hidden = stack[...].astype(BF16)
    latent_part = dot(group_hidden, w_latent[...])
    queries = dot(group_hidden, w_query[...]).astype(BF16)
    query_latent = dot(queries, wk_pad[...])
    queries_f = queries.astype(F32)
    floats = jnp.concatenate(
        [latent_part] + [queries_f[:, h * span + nope : (h + 1) * span] for h in range(heads)],
        axis=1,
    )
    for t in range(nx):
        qmsg_src[t] = query_latent[t * rows : (t + 1) * rows, :].astype(BF16)
        fmsg_src[t] = floats[t * rows : (t + 1) * rows, :]
    qmsg[x] = qmsg_src[x]
    fmsg[x] = fmsg_src[x]
    q_copies = exchange("tp", nx, x, lambda p: qmsg_src.at[p], qmsg, q_send, q_recv)
    f_copies = exchange("tp", nx, x, lambda p: fmsg_src.at[p], fmsg, f_send, f_recv)
    arrived("tp", nx, x, fmsg, f_send, f_recv)
    part = w_latent.shape[1]
    pieces = [fmsg[t] for t in range(nx)]
    latent_full = jnp.concatenate([p[:, :part] for p in pieces], axis=1)
    new_latent = normalize(latent_full, latent_gain[...]).astype(BF16)
    latent_out[...] = new_latent
    for t in range(nx):
        for h in range(heads):
            for s in range(rows):
                n = t * heads + h
                q_rot[s, n : n + 1, :] = pieces[t][
                    s : s + 1, part + h * rope : part + (h + 1) * rope
                ]
    arrived("tp", nx, x, qmsg, q_send, q_recv)
    for t in range(nx):
        values = qmsg[t].astype(F32)
        for h in range(heads):
            for s in range(rows):
                n = t * heads + h
                q_lat[s, n : n + 1, :] = values[s : s + 1, h * rank : (h + 1) * rank]
    lat_copy.wait()
    rop_copy.wait()
    scaling = float(span) ** (-0.5)
    cached = lat.shape[1]
    position = lax.broadcasted_iota(jnp.int32, (nx * heads, cached), 1)
    latent_f = new_latent.astype(F32)
    rope_f = new_rope.astype(F32)
    for s in range(rows):
        ql_f = q_lat[s]
        ql = ql_f.astype(BF16)
        raw = q_rot[s]
        qr = (raw * cos[s : s + 1, :] + swap_halves(raw) * sin[s : s + 1, :]).astype(BF16)
        scores = (dot_nt(ql, lat[s]) + dot(qr, rop[s])) * scaling
        own = jnp.sum(ql_f * latent_f[s : s + 1, :], axis=-1, keepdims=True)
        own = (
            own + jnp.sum(qr.astype(F32) * rope_f[s : s + 1, :], axis=-1, keepdims=True)
        ) * scaling
        scores = jnp.where(position < lengths[s], scores, negative)
        top = jnp.maximum(jnp.max(scores, axis=-1, keepdims=True), own)
        weights = jnp.exp(scores - top)
        own_weight = jnp.exp(own - top)
        total = jnp.sum(weights, axis=-1, keepdims=True) + own_weight
        probs = (weights / total).astype(BF16)
        own_prob = (own_weight / total).astype(BF16).astype(F32)
        got = dot(probs, lat[s]) + own_prob * latent_f[s : s + 1, :]
        for t in range(nx):
            for h in range(heads):
                n = t * heads + h
                att_src_f[t, s : s + 1, h * rank : (h + 1) * rank] = got[n : n + 1, :]
    for t in range(nx):
        att_src[t] = att_src_f[t].astype(BF16)
    att[x] = att_src[x]
    att_copies = exchange("tp", nx, x, lambda p: att_src.at[p], att, att_send, att_recv)
    arrived("tp", nx, x, att, att_send, att_recv)
    for t in range(nx):
        att_stack[t * rows : (t + 1) * rows, :] = att[t].astype(F32)
    attended = att_stack[...].astype(BF16)
    v_head = w_absorb_value.shape[2]
    mixed = jnp.zeros((nx * rows, w_out.shape[1]), F32)
    for h in range(heads):
        head_out = dot(attended[:, h * rank : (h + 1) * rank], w_absorb_value[h]).astype(BF16)
        mixed = mixed + dot(head_out, w_out[h * v_head : (h + 1) * v_head, :])
    for t in range(nx):
        mix_src[t] = mixed[t * rows : (t + 1) * rows, :].astype(BF16)
    mix[x] = mix_src[x]
    mix_copies = exchange("tp", nx, x, lambda p: mix_src.at[p], mix, mix_send, mix_recv)
    arrived("tp", nx, x, mix, mix_send, mix_recv)
    total = mix[0].astype(F32)
    for t in range(1, nx):
        total = total + mix[t].astype(F32)
    residual = (toks + normalize(total, post_gain[...])).astype(BF16)
    residual_out[...] = residual
    ffn_out[...] = normalize(residual, ffn_gain[...]).astype(BF16)
    for copy in hid_copies + q_copies + f_copies + att_copies + mix_copies:
        copy.wait_send()


def expert_kernel(
    sizes,
    ffn_in, residual, routes, route_weights, out_gain, gate_vector,
    w_exp_gate, w_exp_up, w_exp_down, w_dense_gate, w_dense_up, w_dense_down,
    output,
    wg, wu, wd, dg, du, dd, gat0, gat1, stack0, stack1, x0, x1,
    o0, o1, r0, r1, t0, t1, s0, s1,
    w_sem, w_send, w_recv,
    g0_send, g0_recv, g1_send, g1_recv, x0_send, x0_recv, x1_send, x1_recv,
    r0_send, r0_recv, r1_send, r1_recv, s0_send, s0_recv, s1_send, s1_recv,
):
    nz, ny, nc = sizes["ep_0"], sizes["ep_1"], sizes["ep_2"]
    z, y, core = lax.axis_index("ep_0"), lax.axis_index("ep_1"), lax.axis_index("ep_2")
    rows, width = ffn_in.shape
    half = width // 2
    experts = nz * ny * nc
    pairs = (
        (w_exp_gate, wg), (w_exp_up, wu), (w_exp_down, wd),
        (w_dense_gate, dg), (w_dense_up, du), (w_dense_down, dd),
    )
    own_copies = [
        pltpu.make_async_copy(src, dst.at[core], w_sem.at[i])
        for i, (src, dst) in enumerate(pairs)
    ]
    for copy in own_copies:
        copy.start()
    greet((("ep_0", nz), ("ep_1", ny), ("ep_2", nc)))
    other = lax.rem(core + 1, nc)
    far_copies = [
        pltpu.make_async_remote_copy(
            src_ref=src, dst_ref=dst.at[core], send_sem=w_send.at[i], recv_sem=w_recv.at[i],
            device_id={"ep_2": other}, device_id_type=MESH,
        )
        for i, (src, dst) in enumerate(pairs)
    ]
    lane = lax.broadcasted_iota(jnp.int32, (rows, experts), 1)
    chosen = routes[...]
    given = route_weights[...]
    spread = jnp.zeros((rows, experts), F32)
    for k in range(routes.shape[1]):
        spread = spread + jnp.where(lane == chosen[:, k : k + 1], given[:, k : k + 1], 0.0)
    high = spread.astype(BF16)
    low = (spread - high.astype(F32)).astype(BF16)
    gat0[y] = jnp.concatenate([ffn_in[:, :half], high], axis=1)
    gat1[z] = jnp.concatenate([ffn_in[:, half:], low], axis=1)
    copies = exchange("ep_1", ny, y, lambda p: gat0.at[y], gat0, g0_send, g0_recv)
    copies += exchange("ep_0", nz, z, lambda p: gat1.at[z], gat1, g1_send, g1_recv)
    for copy in far_copies:
        copy.start()
    arrived("ep_1", ny, y, gat0, g0_send, g0_recv)
    for i in range(ny):
        stack0[i * rows : (i + 1) * rows, :] = gat0[i].astype(F32)
    x0[z] = stack0[...].astype(BF16)
    copies += exchange("ep_0", nz, z, lambda p: x0.at[z], x0, x0_send, x0_recv)
    arrived("ep_0", nz, z, gat1, g1_send, g1_recv)
    for i in range(nz):
        stack1[i * rows : (i + 1) * rows, :] = gat1[i].astype(F32)
    x1[y] = stack1[...].astype(BF16)
    copies += exchange("ep_1", ny, y, lambda p: x1.at[y], x1, x1_send, x1_recv)
    count = nz * ny * rows
    to = lax.broadcasted_iota(jnp.int32, (count, count), 0)
    fro = lax.broadcasted_iota(jnp.int32, (count, count), 1)
    to_z, to_y, to_r = to // (ny * rows), (to // rows) % ny, to % rows
    swap = jnp.where(fro == to_y * (nz * rows) + to_z * rows + to_r, 1.0, 0.0).astype(BF16)
    swap_back = jnp.where(to == (fro // rows) % ny * (nz * rows) + fro // (ny * rows) * rows + fro % rows, 1.0, 0.0).astype(BF16)
    for copy in own_copies:
        copy.wait()
    for copy in far_copies:
        copy.wait()
    arrived("ep_0", nz, z, x0, x0_send, x0_recv)
    arrived("ep_1", ny, y, x1, x1_send, x1_recv)
    first = x0[...].reshape(count, half + experts)
    second = dot(swap, x1[...].reshape(count, half + experts)).astype(BF16)
    every = jnp.concatenate([first[:, :half], second[:, :half]], axis=1)
    spread = first[:, half:].astype(F32) + second[:, half:].astype(F32)
    columns = lax.broadcasted_iota(jnp.int32, (count, experts), 1)
    chip = (z * ny + y) * nc
    acts = []
    for e in range(nc):
        weight = jnp.sum(jnp.where(columns == chip + e, spread, 0.0), axis=1, keepdims=True)
        act = silu(dot(every, wg[e, 0])) * dot(every, wu[e, 0])
        acts.append((act * weight).astype(BF16))
    acts = jnp.concatenate(acts, axis=1)
    gate = jnp.sum(every.astype(F32) * gate_vector[...], axis=1, keepdims=True)
    gate = 1.0 / (1.0 + jnp.exp(-gate))
    units = nc * dg.shape[1]
    dense = silu(dot_nt(every, dg[...].reshape(units, width))) * dot_nt(
        every, du[...].reshape(units, width)
    )
    dense = (dense * gate).astype(BF16)
    down = wd[...].reshape(nc * wd.shape[2], width)
    dense_down = dd[...].reshape(units, width)
    part0 = dot(acts, down[:, :half]) + dot(dense, dense_down[:, :half])
    o0[...] = part0.astype(BF16).reshape(o0.shape)
    copies += exchange("ep_0", nz, z, lambda p: o0.at[p], r0, r0_send, r0_recv)
    acts_swapped = dot(swap_back, acts).astype(BF16)
    dense_swapped = dot(swap_back, dense).astype(BF16)
    part1 = dot(acts_swapped, down[:, half:]) + dot(dense_swapped, dense_down[:, half:])
    o1[...] = part1.astype(BF16).reshape(o1.shape)
    copies += exchange("ep_1", ny, y, lambda p: o1.at[p], r1, r1_send, r1_recv)
    r0[z] = o0[z]
    r1[y] = o1[y]
    arrived("ep_0", nz, z, r0, r0_send, r0_recv)
    total = r0[0].astype(F32)
    for i in range(1, nz):
        total = total + r0[i].astype(F32)
    for i in range(ny):
        t0[i] = total[i * rows : (i + 1) * rows, :].astype(BF16)
    copies += exchange("ep_1", ny, y, lambda p: t0.at[p], s0, s0_send, s0_recv)
    arrived("ep_1", ny, y, r1, r1_send, r1_recv)
    total = r1[0].astype(F32)
    for i in range(1, ny):
        total = total + r1[i].astype(F32)
    for i in range(nz):
        t1[i] = total[i * rows : (i + 1) * rows, :].astype(BF16)
    copies += exchange("ep_0", nz, z, lambda p: t1.at[p], s1, s1_send, s1_recv)
    s0[y] = t0[y]
    s1[z] = t1[z]
    arrived("ep_1", ny, y, s0, s0_send, s0_recv)
    arrived("ep_0", nz, z, s1, s1_send, s1_recv)
    left = s0[0].astype(F32)
    for i in range(1, ny):
        left = left + s0[i].astype(F32)
    right = s1[0].astype(F32)
    for i in range(1, nz):
        right = right + s1[i].astype(F32)
    combined = jnp.concatenate([left, right], axis=1)
    output[...] = (residual[...].astype(F32) + normalize(combined, out_gain[...])).astype(BF16)
    for copy in copies:
        copy.wait_send()


def in_vmem(count):
    return [pl.BlockSpec(memory_space=pltpu.VMEM)] * count


def in_place(count):
    return [pl.BlockSpec(memory_space=pl.ANY)] * count


def semaphores(*counts):
    return [pltpu.SemaphoreType.DMA((n,)) for n in counts]


def shards(
    sizes,
    tokens,
    lengths,
    cache_latent,
    cache_rope,
    attn_gain,
    latent_gain,
    post_gain,
    ffn_gain,
    out_gain,
    w_latent,
    w_rope_key,
    w_query,
    w_absorb_key,
    w_absorb_value,
    w_out,
    routes,
    route_weights,
    w_exp_gate,
    w_exp_up,
    w_exp_down,
    w_dense_gate,
    w_dense_up,
    w_dense_down,
    dense_gate_vector,
):
    rows, width = tokens.shape
    nz, ny, nc, nx = sizes["ep_0"], sizes["ep_1"], sizes["ep_2"], sizes["tp"]
    half = width // 2
    experts = nz * ny * nc
    heads, nope, rank = w_absorb_key.shape
    rope = w_rope_key.shape[1]
    part = w_latent.shape[1]
    floats = part + heads * rope
    inverse = rope_base ** (-jnp.arange(rope // 2, dtype=F32) / (rope // 2))
    angles = lengths.astype(F32)[:, None] * inverse
    cosines = jnp.concatenate([jnp.cos(angles)] * 2, axis=1)
    sine = jnp.sin(angles)
    sines = jnp.concatenate([-sine, sine], axis=1)
    V = pltpu.VMEM
    residual, ffn_in, new_latent, new_rope = pl.pallas_call(
        functools.partial(attention_kernel, sizes),
        out_shape=(
            jax.ShapeDtypeStruct((rows, width), BF16),
            jax.ShapeDtypeStruct((rows, width), BF16),
            jax.ShapeDtypeStruct((rows, rank), BF16),
            jax.ShapeDtypeStruct((rows, rope), BF16),
        ),
        in_specs=[pl.BlockSpec(memory_space=pltpu.SMEM)] + in_vmem(13) + in_place(2),
        out_specs=tuple(in_vmem(4)),
        scratch_shapes=[
            V(cache_latent.shape, BF16),
            V(cache_rope.shape, BF16),
            V((nx, rows, width), BF16),
            V((nx * rows, width), F32),
            V((nx, rows, heads * rank), BF16),
            V((nx, rows, heads * rank), BF16),
            V((nx, rows, floats), F32),
            V((nx, rows, floats), F32),
            V((w_query.shape[1], heads * rank), BF16),
            V((rows, nx * heads, rank), F32),
            V((rows, nx * heads, rope), F32),
            V((nx, rows, heads * rank), F32),
            V((nx, rows, heads * rank), BF16),
            V((nx, rows, heads * rank), BF16),
            V((nx * rows, heads * rank), F32),
            V((nx, rows, width), BF16),
            V((nx, rows, width), BF16),
        ]
        + semaphores(2, *([nx - 1, nx] * 5)),
        compiler_params=pltpu.CompilerParams(collective_id=0, has_side_effects=True),
        cost_estimate=pl.CostEstimate(flops=10**8, bytes_accessed=4 * 10**6, transcendentals=0),
        name="attention",
    )(
        lengths, tokens, cosines, sines, attn_gain[None], latent_gain[None], post_gain[None],
        ffn_gain[None], w_latent, w_rope_key, w_query, w_absorb_key, w_absorb_value, w_out,
        cache_latent, cache_rope,
    )
    output = pl.pallas_call(
        functools.partial(expert_kernel, sizes),
        out_shape=jax.ShapeDtypeStruct((rows, width), BF16),
        in_specs=in_vmem(6) + in_place(6),
        out_specs=in_vmem(1)[0],
        scratch_shapes=[
            V((nc, *w_exp_gate.shape), BF16),
            V((nc, *w_exp_up.shape), BF16),
            V((nc, *w_exp_down.shape), BF16),
            V((nc, *w_dense_gate.shape), BF16),
            V((nc, *w_dense_up.shape), BF16),
            V((nc, *w_dense_down.shape), BF16),
            V((ny, rows, half + experts), BF16),
            V((nz, rows, half + experts), BF16),
            V((ny * rows, half + experts), F32),
            V((nz * rows, half + experts), F32),
            V((nz, ny * rows, half + experts), BF16),
            V((ny, nz * rows, half + experts), BF16),
            V((nz, ny * rows, half), BF16),
            V((ny, nz * rows, half), BF16),
            V((nz, ny * rows, half), BF16),
            V((ny, nz * rows, half), BF16),
            V((ny, rows, half), BF16),
            V((nz, rows, half), BF16),
            V((ny, rows, half), BF16),
            V((nz, rows, half), BF16),
        ]
        + semaphores(6, 6, 6, *([ny - 1, ny, nz - 1, nz, nz - 1, nz, ny - 1, ny] * 2)),
        compiler_params=pltpu.CompilerParams(collective_id=1, has_side_effects=True),
        cost_estimate=pl.CostEstimate(flops=10**9, bytes_accessed=4 * 10**6, transcendentals=0),
        name="experts",
    )(
        ffn_in, residual, routes, route_weights, out_gain[None], dense_gate_vector[None],
        w_exp_gate, w_exp_up, w_exp_down, w_dense_gate, w_dense_up, w_dense_down,
    )
    return (output, new_latent, new_rope)


def solution(mesh, dims=(8, 8, 2)):
    torus = Mesh(mesh.devices.reshape(*dims, mesh.shape["tp"]), EP_TP)
    placed = (
        P(EP_TP, None),
        P(EP_TP),
        P(EP_TP, None, None),
        P(EP_TP, None, None),
        P(),
        P(),
        P(),
        P(),
        P(),
        P(None, "tp"),
        P(),
        P(None, "tp"),
        P("tp", None, None),
        P("tp", None, None),
        P("tp", None),
        P(EP_TP, None),
        P(EP_TP, None),
        P(EP, None, None),
        P(EP, None, None),
        P(EP, None, None),
        P(EP, None),
        P(EP, None),
        P(EP, None),
        P(),
    )
    return jax.shard_map(
        functools.partial(shards, dict(torus.shape)),
        mesh=torus,
        in_specs=placed,
        out_specs=(P(EP_TP, None), P(EP_TP, None), P(EP_TP, None)),
        check_vma=False,
    )
```

```python
import functools

import jax
import jax.numpy as jnp
import numpy as np
from jax import lax
from jax.experimental import pallas as pl
from jax.experimental.pallas import tpu as pltpu
from jax.sharding import Mesh
from jax.sharding import PartitionSpec as P

EP = ("ep_0", "ep_1", "ep_2")
EP_TP = ("ep_0", "ep_1", "ep_2", "tp")
MESH = pl.DeviceIdType.MESH
F32 = jnp.float32
BF16 = jnp.bfloat16

epsilon = 1e-06
rope_base = 10000.0
negative = -1e30


def dot(a, b):
    return jnp.dot(a, b, preferred_element_type=F32)


def dot_nt(a, b):
    return lax.dot_general(a, b, (((1,), (1,)), ((), ())), preferred_element_type=F32)


def normalize(values, gain):
    values = values.astype(F32)
    mean = jnp.mean(values * values, axis=-1, keepdims=True)
    return values * lax.rsqrt(mean + epsilon) * gain


def swap_halves(values):
    half = values.shape[-1] // 2
    return jnp.concatenate([values[:, half:], values[:, :half]], axis=1)


def silu(values):
    return values / (1.0 + jnp.exp(-values))


def exchange(axis, size, me, src_of, dst, send, recv):
    copies = []
    for k in range(1, size):
        partner = lax.rem(me + k, size)
        copy = pltpu.make_async_remote_copy(
            src_ref=src_of(partner),
            dst_ref=dst.at[me],
            send_sem=send.at[k - 1],
            recv_sem=recv.at[me],
            device_id={axis: partner},
            device_id_type=MESH,
        )
        copy.start()
        copies.append(copy)
    return copies


def arrived(axis, size, me, dst, send, recv):
    for k in range(1, size):
        partner = lax.rem(me + k, size)
        pltpu.make_async_remote_copy(
            src_ref=dst.at[partner],
            dst_ref=dst.at[partner],
            send_sem=send.at[k - 1],
            recv_sem=recv.at[partner],
            device_id={axis: partner},
            device_id_type=MESH,
        ).wait_recv()


def greet(axes):
    barrier = pltpu.get_barrier_semaphore()
    total = 0
    for axis, size in axes:
        me = lax.axis_index(axis)
        for k in range(1, size):
            pl.semaphore_signal(
                barrier,
                inc=1,
                device_id={axis: lax.rem(me + k, size)},
                device_id_type=MESH,
            )
            total += 1
    return barrier, total


def stack_rows(blocks, stack, count, rows):
    for i in range(count):
        stack[i * rows : (i + 1) * rows, :] = blocks[i].astype(F32)
    return stack[...].astype(BF16)


def added(blocks, count):
    total = blocks[0].astype(F32)
    for i in range(1, count):
        total = total + blocks[i].astype(F32)
    return total


def layer_kernel(
    sizes,
    stop,
    lengths, tokens_in, inverse_in, attn_gain_in, latent_gain_in, post_gain_in, ffn_gain_in,
    out_gain_in, gate_vector_in, routes_in, route_weights_in,
    w_latent, w_rope_key, w_query, w_absorb_key, w_absorb_value, w_out,
    cache_latent, cache_rope,
    w_exp_gate, w_exp_up, w_exp_down, w_dense_gate, w_dense_up, w_dense_down,
    output, latent_out, rope_out,
    tokens, inverse, attn_gain, latent_gain, post_gain, ffn_gain, out_gain, gate_vector,
    routes, route_weights, w_front, w_rope, wk, wv, wo, lat, rop, wg, wu, wd, dg, du, dd,
    hid, stack, qmsg_src, qmsg, fmsg_src, fmsg, wk_pad, q_lat, q_rot,
    att_src_f, att_src, att, att_stack, mix_src, mix,
    gw0, gw1, stack_w0, stack_w1, w0, w1, gat0, gat1, stack0, stack1, x0, x1,
    o0, o1, r0, r1, t0, t1, s0, s1,
    in_sem, far_send, far_recv,
    hid_send, hid_recv, q_send, q_recv, f_send, f_recv,
    att_send, att_recv, mix_send, mix_recv,
    gw0_send, gw0_recv, gw1_send, gw1_recv, w0_send, w0_recv, w1_send, w1_recv,
    g0_send, g0_recv, g1_send, g1_recv, x0_send, x0_recv, x1_send, x1_recv,
    r0_send, r0_recv, r1_send, r1_recv, s0_send, s0_recv, s1_send, s1_recv,
):
    nz, ny, nc, nx = sizes["ep_0"], sizes["ep_1"], sizes["ep_2"], sizes["tp"]
    z, y, core = lax.axis_index("ep_0"), lax.axis_index("ep_1"), lax.axis_index("ep_2")
    x = lax.axis_index("tp")
    rows, width = tokens.shape
    half = width // 2
    experts = nz * ny * nc
    heads, nope, rank = w_absorb_key.shape
    part = w_latent.shape[0]
    rope = w_rope_key.shape[0]
    span = nope + rope
    barrier, total = greet((("tp", nx), ("ep_2", nc), ("ep_1", ny), ("ep_0", nz)))

    moves = [
        (tokens_in, tokens), (attn_gain_in, attn_gain),
        (routes_in, routes), (route_weights_in, route_weights), (inverse_in, inverse),
    ]
    front = [(w_rope_key, w_rope)]
    for h in range(heads):
        front.append((w_query.at[pl.ds(h * span, nope)], w_front.at[pl.ds(h * nope, nope)]))
    front.append((w_latent, w_front.at[pl.ds(heads * nope, part)]))
    for h in range(heads):
        front.append(
            (
                w_query.at[pl.ds(h * span + nope, rope)],
                w_front.at[pl.ds(heads * nope + part + h * rope, rope)],
            )
        )
    front.append((w_absorb_key, wk))
    middle = [
        (latent_gain_in, latent_gain), (cache_latent, lat), (cache_rope, rop),
        (w_absorb_value, wv), (w_out, wo), (post_gain_in, post_gain), (ffn_gain_in, ffn_gain),
        (out_gain_in, out_gain), (gate_vector_in, gate_vector),
    ]
    pairs = [
        (w_exp_gate, wg), (w_exp_up, wu), (w_exp_down, wd),
        (w_dense_gate, dg), (w_dense_up, du), (w_dense_down, dd),
    ]
    back = [(src, dst.at[core]) for src, dst in pairs]
    started = []
    for src, dst in moves + front + middle + back:
        copy = pltpu.make_async_copy(src, dst, in_sem.at[len(started)])
        copy.start()
        started.append(copy)
    waiting = iter(started)

    def take(count):
        for _ in range(count):
            next(waiting).wait()

    take(len(moves))
    toks = tokens[...].astype(F32)
    hidden = normalize(toks, attn_gain[...]).astype(BF16)
    hid[x] = hidden
    lane = lax.broadcasted_iota(jnp.int32, (rows, experts), 1)
    chosen = routes[...]
    given = route_weights[...]
    spread = jnp.zeros((rows, experts), F32)
    for k in range(routes.shape[1]):
        spread = spread + jnp.where(lane == chosen[:, k : k + 1], given[:, k : k + 1], 0.0)
    high = spread.astype(BF16)
    gw0[y] = high
    gw1[z] = (spread - high.astype(F32)).astype(BF16)

    pl.semaphore_wait(barrier, total)
    sent = []

    def finish():
        for copy in waiting:
            copy.wait()
        for copy in sent:
            copy.wait_send()
        output[...] = toks.astype(BF16)

    sent += exchange("tp", nx, x, lambda p: hid.at[x], hid, hid_send, hid_recv)
    other = lax.rem(core + 1, nc)
    far = [
        pltpu.make_async_remote_copy(
            src_ref=src, dst_ref=dst.at[core], send_sem=far_send.at[i], recv_sem=far_recv.at[i],
            device_id={"ep_2": other}, device_id_type=MESH,
        )
        for i, (src, dst) in enumerate(pairs)
    ]
    for copy in far:
        copy.start()
    sent += exchange("ep_1", ny, y, lambda p: gw0.at[y], gw0, gw0_send, gw0_recv)
    sent += exchange("ep_0", nz, z, lambda p: gw1.at[z], gw1, gw1_send, gw1_recv)

    row = lax.broadcasted_iota(jnp.int32, (rows, rope), 0)
    held = jnp.zeros((rows, rope), F32)
    for s in range(rows):
        held = jnp.where(row == s, lengths[s].astype(F32), held)
    angles = held * inverse[...]
    cos = jnp.cos(angles)
    sin = jnp.sin(angles)
    first_half = lax.broadcasted_iota(jnp.int32, (rows, rope), 1) < rope // 2
    sin = jnp.where(first_half, -sin, sin)
    wk_pad[...] = jnp.zeros(wk_pad.shape, BF16)
    take(len(front))
    for h in range(heads):
        wk_pad[h * nope : (h + 1) * nope, h * rank : (h + 1) * rank] = wk[h]
    rope_pre = dot_nt(hidden, w_rope[...])
    new_rope = (rope_pre * cos + swap_halves(rope_pre) * sin).astype(BF16)
    rope_out[...] = new_rope
    arrived("tp", nx, x, hid, hid_send, hid_recv)
    if stop == 1:
        for copy in far:
            copy.wait()
        arrived("ep_1", ny, y, gw0, gw0_send, gw0_recv)
        arrived("ep_0", nz, z, gw1, gw1_send, gw1_recv)
        return finish()
    projected = dot_nt(stack_rows(hid, stack, nx, rows), w_front[...])
    flat = heads * nope
    query_latent = dot(projected[:, :flat].astype(BF16), wk_pad[...])
    for t in range(nx):
        qmsg_src[t] = query_latent[t * rows : (t + 1) * rows, :].astype(BF16)
        fmsg_src[t] = projected[t * rows : (t + 1) * rows, flat:]
    sent += exchange("tp", nx, x, lambda p: fmsg_src.at[p], fmsg, f_send, f_recv)
    sent += exchange("tp", nx, x, lambda p: qmsg_src.at[p], qmsg, q_send, q_recv)
    qmsg[x] = qmsg_src[x]
    fmsg[x] = fmsg_src[x]
    arrived("ep_1", ny, y, gw0, gw0_send, gw0_recv)
    arrived("ep_0", nz, z, gw1, gw1_send, gw1_recv)
    w0[z] = stack_rows(gw0, stack_w0, ny, rows)
    w1[y] = stack_rows(gw1, stack_w1, nz, rows)
    arrived("tp", nx, x, fmsg, f_send, f_recv)
    pieces = [fmsg[t] for t in range(nx)]
    latent_full = jnp.concatenate([p[:, :part] for p in pieces], axis=1)
    take(len(middle))
    new_latent = normalize(latent_full, latent_gain[...]).astype(BF16)
    latent_out[...] = new_latent
    for t in range(nx):
        values = pieces[t].astype(BF16).astype(F32)
        for h in range(heads):
            for s in range(rows):
                n = t * heads + h
                q_rot[s, n : n + 1, :] = values[
                    s : s + 1, part + h * rope : part + (h + 1) * rope
                ]
    arrived("tp", nx, x, qmsg, q_send, q_recv)
    sent += exchange("ep_0", nz, z, lambda p: w0.at[z], w0, w0_send, w0_recv)
    sent += exchange("ep_1", ny, y, lambda p: w1.at[y], w1, w1_send, w1_recv)
    for t in range(nx):
        values = qmsg[t].astype(F32)
        for h in range(heads):
            for s in range(rows):
                n = t * heads + h
                q_lat[s, n : n + 1, :] = values[s : s + 1, h * rank : (h + 1) * rank]

    def early():
        for copy in far:
            copy.wait()
        arrived("ep_0", nz, z, w0, w0_send, w0_recv)
        arrived("ep_1", ny, y, w1, w1_send, w1_recv)

    if stop == 2:
        early()
        return finish()
    scaling = float(span) ** (-0.5)
    cached = lat.shape[1]
    position = lax.broadcasted_iota(jnp.int32, (nx * heads, cached), 1)
    latent_f = new_latent.astype(F32)
    rope_f = new_rope.astype(F32)
    for s in range(rows):
        ql_f = q_lat[s]
        raw = q_rot[s]
        qr = (raw * cos[s : s + 1, :] + swap_halves(raw) * sin[s : s + 1, :]).astype(BF16)
        scores = (dot_nt(ql_f.astype(BF16), lat[s]) + dot(qr, rop[s])) * scaling
        own = jnp.sum(ql_f * latent_f[s : s + 1, :], axis=-1, keepdims=True)
        own = (
            own + jnp.sum(qr.astype(F32) * rope_f[s : s + 1, :], axis=-1, keepdims=True)
        ) * scaling
        scores = jnp.where(position < lengths[s], scores, negative)
        top = jnp.maximum(jnp.max(scores, axis=-1, keepdims=True), own)
        weights = jnp.exp(scores - top)
        own_weight = jnp.exp(own - top)
        whole = jnp.sum(weights, axis=-1, keepdims=True) + own_weight
        probs = (weights / whole).astype(BF16)
        own_prob = (own_weight / whole).astype(BF16).astype(F32)
        got = dot(probs, lat[s]) + own_prob * latent_f[s : s + 1, :]
        for t in range(nx):
            for h in range(heads):
                n = t * heads + h
                att_src_f[t, s : s + 1, h * rank : (h + 1) * rank] = got[n : n + 1, :]
    for t in range(nx):
        att_src[t] = att_src_f[t].astype(BF16)
    sent += exchange("tp", nx, x, lambda p: att_src.at[p], att, att_send, att_recv)
    att[x] = att_src[x]
    if stop == 3:
        arrived("tp", nx, x, att, att_send, att_recv)
        early()
        return finish()
    count = nz * ny * rows
    to = lax.broadcasted_iota(jnp.int32, (count, count), 0)
    fro = lax.broadcasted_iota(jnp.int32, (count, count), 1)
    source = to // rows % ny * (nz * rows) + to // (ny * rows) * rows + to % rows
    swap = jnp.where(fro == source, 1.0, 0.0).astype(BF16)
    source = fro // rows % ny * (nz * rows) + fro // (ny * rows) * rows + fro % rows
    swap_back = jnp.where(to == source, 1.0, 0.0).astype(BF16)
    early()
    spread = w0[...].reshape(count, experts).astype(F32) + dot(
        swap, w1[...].reshape(count, experts)
    )
    columns = lax.broadcasted_iota(jnp.int32, (count, experts), 1)
    chip = (z * ny + y) * nc
    shares = [
        jnp.sum(jnp.where(columns == chip + e, spread, 0.0), axis=1, keepdims=True)
        for e in range(nc)
    ]
    arrived("tp", nx, x, att, att_send, att_recv)
    attended = stack_rows(att, att_stack, nx, rows)
    v_head = wv.shape[1]
    mixed = jnp.zeros((nx * rows, width), F32)
    for h in range(heads):
        head_out = dot_nt(attended[:, h * rank : (h + 1) * rank], wv[h]).astype(BF16)
        mixed = mixed + dot(head_out, wo[h * v_head : (h + 1) * v_head, :])
    for t in range(nx):
        mix_src[t] = mixed[t * rows : (t + 1) * rows, :].astype(BF16)
    sent += exchange("tp", nx, x, lambda p: mix_src.at[p], mix, mix_send, mix_recv)
    mix[x] = mix_src[x]
    arrived("tp", nx, x, mix, mix_send, mix_recv)
    if stop == 4:
        return finish()
    residual = (toks + normalize(added(mix, nx), post_gain[...])).astype(BF16)
    ffn_in = normalize(residual, ffn_gain[...]).astype(BF16)

    gat0[y] = ffn_in[:, :half]
    gat1[z] = ffn_in[:, half:]
    sent += exchange("ep_1", ny, y, lambda p: gat0.at[y], gat0, g0_send, g0_recv)
    sent += exchange("ep_0", nz, z, lambda p: gat1.at[z], gat1, g1_send, g1_recv)
    arrived("ep_1", ny, y, gat0, g0_send, g0_recv)
    x0[z] = stack_rows(gat0, stack0, ny, rows)
    sent += exchange("ep_0", nz, z, lambda p: x0.at[z], x0, x0_send, x0_recv)
    arrived("ep_0", nz, z, gat1, g1_send, g1_recv)
    x1[y] = stack_rows(gat1, stack1, nz, rows)
    sent += exchange("ep_1", ny, y, lambda p: x1.at[y], x1, x1_send, x1_recv)
    if stop == 5:
        arrived("ep_0", nz, z, x0, x0_send, x0_recv)
        arrived("ep_1", ny, y, x1, x1_send, x1_recv)
        return finish()
    take(len(back))
    arrived("ep_0", nz, z, x0, x0_send, x0_recv)
    arrived("ep_1", ny, y, x1, x1_send, x1_recv)
    first = x0[...].reshape(count, half)
    second = dot(swap, x1[...].reshape(count, half)).astype(BF16)
    every = jnp.concatenate([first, second], axis=1)
    acts = []
    for e in range(nc):
        act = silu(dot(every, wg[e, 0])) * dot(every, wu[e, 0])
        acts.append((act * shares[e]).astype(BF16))
    acts = jnp.concatenate(acts, axis=1)
    gate = jnp.sum(every.astype(F32) * gate_vector[...], axis=1, keepdims=True)
    gate = 1.0 / (1.0 + jnp.exp(-gate))
    units = nc * dg.shape[1]
    dense = silu(dot_nt(every, dg[...].reshape(units, width))) * dot_nt(
        every, du[...].reshape(units, width)
    )
    dense = (dense * gate).astype(BF16)
    down = wd[...].reshape(nc * wd.shape[2], width)
    dense_down = dd[...].reshape(units, width)
    part0 = dot(acts, down[:, :half]) + dot(dense, dense_down[:, :half])
    o0[...] = part0.astype(BF16).reshape(o0.shape)
    sent += exchange("ep_0", nz, z, lambda p: o0.at[p], r0, r0_send, r0_recv)
    acts_swapped = dot(swap_back, acts).astype(BF16)
    dense_swapped = dot(swap_back, dense).astype(BF16)
    part1 = dot(acts_swapped, down[:, half:]) + dot(dense_swapped, dense_down[:, half:])
    o1[...] = part1.astype(BF16).reshape(o1.shape)
    if stop == 6:
        arrived("ep_0", nz, z, r0, r0_send, r0_recv)
        return finish()
    sent += exchange("ep_1", ny, y, lambda p: o1.at[p], r1, r1_send, r1_recv)
    r0[z] = o0[z]
    r1[y] = o1[y]
    arrived("ep_0", nz, z, r0, r0_send, r0_recv)
    if stop == 7:
        arrived("ep_1", ny, y, r1, r1_send, r1_recv)
        return finish()
    whole = added(r0, nz)
    for i in range(ny):
        t0[i] = whole[i * rows : (i + 1) * rows, :].astype(BF16)
    sent += exchange("ep_1", ny, y, lambda p: t0.at[p], s0, s0_send, s0_recv)
    arrived("ep_1", ny, y, r1, r1_send, r1_recv)
    whole = added(r1, ny)
    for i in range(nz):
        t1[i] = whole[i * rows : (i + 1) * rows, :].astype(BF16)
    sent += exchange("ep_0", nz, z, lambda p: t1.at[p], s1, s1_send, s1_recv)
    s0[y] = t0[y]
    s1[z] = t1[z]
    arrived("ep_1", ny, y, s0, s0_send, s0_recv)
    arrived("ep_0", nz, z, s1, s1_send, s1_recv)
    combined = jnp.concatenate([added(s0, ny), added(s1, nz)], axis=1)
    output[...] = (residual.astype(F32) + normalize(combined, out_gain[...])).astype(BF16)
    for copy in sent:
        copy.wait_send()


def tail_kernel(a, b, c, a_out, b_out, c_out):
    a_out[...] = a[...]
    b_out[...] = b[...]
    c_out[...] = c[...]


def in_vmem(count):
    return [pl.BlockSpec(memory_space=pltpu.VMEM)] * count


def in_place(count):
    return [pl.BlockSpec(memory_space=pl.ANY)] * count


def semaphores(*counts):
    return [pltpu.SemaphoreType.DMA((n,)) for n in counts]


def shards(
    sizes,
    stop,
    tokens,
    lengths,
    cache_latent,
    cache_rope,
    attn_gain,
    latent_gain,
    post_gain,
    ffn_gain,
    out_gain,
    w_latent,
    w_rope_key,
    w_query,
    w_absorb_key,
    w_absorb_value,
    w_out,
    routes,
    route_weights,
    w_exp_gate,
    w_exp_up,
    w_exp_down,
    w_dense_gate,
    w_dense_up,
    w_dense_down,
    dense_gate_vector,
):
    rows, width = tokens.shape
    nz, ny, nc, nx = sizes["ep_0"], sizes["ep_1"], sizes["ep_2"], sizes["tp"]
    half = width // 2
    experts = nz * ny * nc
    heads, nope, rank = w_absorb_key.shape
    rope = w_rope_key.shape[1]
    part = w_latent.shape[1]
    floats = part + heads * rope
    inverse = np.float32(rope_base) ** (-np.arange(rope // 2, dtype=np.float32) / (rope // 2))
    inverse = np.concatenate([inverse, inverse])[None]
    V = pltpu.VMEM
    weights = (w_exp_gate, w_exp_up, w_exp_down, w_dense_gate, w_dense_up, w_dense_down)
    outs = (
        jax.ShapeDtypeStruct((rows, width), BF16),
        jax.ShapeDtypeStruct((rows, rank), BF16),
        jax.ShapeDtypeStruct((rows, rope), BF16),
    )
    args = (
        lengths, tokens, jnp.asarray(inverse), attn_gain[None], latent_gain[None], post_gain[None],
        ffn_gain[None], out_gain[None], dense_gate_vector[None], routes, route_weights,
        w_latent.T, w_rope_key.T, w_query.T, w_absorb_key, jnp.swapaxes(w_absorb_value, 1, 2),
        w_out, cache_latent, cache_rope, *weights,
    )
    plane = [ny - 1, ny, nz - 1, nz, nz - 1, nz, ny - 1, ny]
    results = pl.pallas_call(
        functools.partial(layer_kernel, sizes, stop),
        out_shape=outs,
        in_specs=[pl.BlockSpec(memory_space=pltpu.SMEM)] + in_place(len(args) - 1),
        out_specs=tuple(in_vmem(3)),
        scratch_shapes=[
            V((rows, width), BF16),
            V((1, rope), F32),
            V((1, width), F32),
            V((1, rank), F32),
            V((1, width), F32),
            V((1, width), F32),
            V((1, width), F32),
            V((1, width), F32),
            V(routes.shape, jnp.int32),
            V(route_weights.shape, F32),
            V((heads * nope + floats, width), BF16),
            V((rope, width), BF16),
            V(w_absorb_key.shape, BF16),
            V((heads, w_absorb_value.shape[2], rank), BF16),
            V(w_out.shape, BF16),
            V(cache_latent.shape, BF16),
            V(cache_rope.shape, BF16),
            *[V((nc, *w.shape), BF16) for w in weights],
            V((nx, rows, width), BF16),
            V((nx * rows, width), F32),
            V((nx, rows, heads * rank), BF16),
            V((nx, rows, heads * rank), BF16),
            V((nx, rows, floats), F32),
            V((nx, rows, floats), F32),
            V((heads * nope, heads * rank), BF16),
            V((rows, nx * heads, rank), F32),
            V((rows, nx * heads, rope), F32),
            V((nx, rows, heads * rank), F32),
            V((nx, rows, heads * rank), BF16),
            V((nx, rows, heads * rank), BF16),
            V((nx * rows, heads * rank), F32),
            V((nx, rows, width), BF16),
            V((nx, rows, width), BF16),
            V((ny, rows, experts), BF16),
            V((nz, rows, experts), BF16),
            V((ny * rows, experts), F32),
            V((nz * rows, experts), F32),
            V((nz, ny * rows, experts), BF16),
            V((ny, nz * rows, experts), BF16),
            V((ny, rows, half), BF16),
            V((nz, rows, half), BF16),
            V((ny * rows, half), F32),
            V((nz * rows, half), F32),
            V((nz, ny * rows, half), BF16),
            V((ny, nz * rows, half), BF16),
            V((nz, ny * rows, half), BF16),
            V((ny, nz * rows, half), BF16),
            V((nz, ny * rows, half), BF16),
            V((ny, nz * rows, half), BF16),
            V((ny, rows, half), BF16),
            V((nz, rows, half), BF16),
            V((ny, rows, half), BF16),
            V((nz, rows, half), BF16),
        ]
        + semaphores(40, 6, 6, *([nx - 1, nx] * 5), *(plane * 3)),
        compiler_params=pltpu.CompilerParams(collective_id=0, has_side_effects=True),
        name="layer",
    )(*args)
    return pl.pallas_call(
        tail_kernel,
        out_shape=outs,
        in_specs=in_vmem(3),
        out_specs=tuple(in_vmem(3)),
        name="tail",
    )(*results)


def solution(mesh, dims=(8, 8, 2), stop=0):
    torus = Mesh(mesh.devices.reshape(*dims, mesh.shape["tp"]), EP_TP)
    placed = (
        P(EP_TP, None),
        P(EP_TP),
        P(EP_TP, None, None),
        P(EP_TP, None, None),
        P(),
        P(),
        P(),
        P(),
        P(),
        P(None, "tp"),
        P(),
        P(None, "tp"),
        P("tp", None, None),
        P("tp", None, None),
        P("tp", None),
        P(EP_TP, None),
        P(EP_TP, None),
        P(EP, None, None),
        P(EP, None, None),
        P(EP, None, None),
        P(EP, None),
        P(EP, None),
        P(EP, None),
        P(),
    )
    return jax.shard_map(
        functools.partial(shards, dict(torus.shape), stop),
        mesh=torus,
        in_specs=placed,
        out_specs=(P(EP_TP, None), P(EP_TP, None), P(EP_TP, None)),
        check_vma=False,
    )
```

```python
import functools

import jax
import jax.numpy as jnp
import numpy as np
from jax import lax
from jax.experimental import pallas as pl
from jax.experimental.pallas import tpu as pltpu
from jax.sharding import Mesh
from jax.sharding import PartitionSpec as P

EP = ("ep_0", "ep_1", "ep_2")
EP_TP = ("ep_0", "ep_1", "ep_2", "tp")
MESH = pl.DeviceIdType.MESH
F32 = jnp.float32
BF16 = jnp.bfloat16

epsilon = 1e-06
rope_base = 10000.0
negative = -1e30


def dot(a, b):
    return jnp.dot(a, b, preferred_element_type=F32)


def dot_nt(a, b):
    return lax.dot_general(a, b, (((1,), (1,)), ((), ())), preferred_element_type=F32)


def normalize(values, gain):
    values = values.astype(F32)
    mean = jnp.mean(values * values, axis=-1, keepdims=True)
    return values * lax.rsqrt(mean + epsilon) * gain


def swap_halves(values):
    half = values.shape[-1] // 2
    return jnp.concatenate([values[:, half:], values[:, :half]], axis=1)


def silu(values):
    return values / (1.0 + jnp.exp(-values))


def exchange(axis, size, me, src_of, dst, send, recv):
    copies = []
    for k in range(1, size):
        partner = lax.rem(me + k, size)
        copy = pltpu.make_async_remote_copy(
            src_ref=src_of(partner),
            dst_ref=dst.at[me],
            send_sem=send.at[k - 1],
            recv_sem=recv.at[me],
            device_id={axis: partner},
            device_id_type=MESH,
        )
        copy.start()
        copies.append(copy)
    return copies


def arrived(axis, size, me, dst, send, recv):
    for k in range(1, size):
        partner = lax.rem(me + k, size)
        pltpu.make_async_remote_copy(
            src_ref=dst.at[partner],
            dst_ref=dst.at[partner],
            send_sem=send.at[k - 1],
            recv_sem=recv.at[partner],
            device_id={axis: partner},
            device_id_type=MESH,
        ).wait_recv()


def offsets(size):
    order = [0]
    for k in range(1, (size + 1) // 2):
        order += [k, -k]
    if size % 2 == 0:
        order.append(size // 2)
    return order, [order.index(-k if -k in order else k) for k in order]


def ring_copy(where, size, off, src, dst, send, recv):
    return pltpu.make_async_remote_copy(
        src_ref=src, dst_ref=dst, send_sem=send, recv_sem=recv,
        device_id=where(off), device_id_type=MESH,
    )


def ring_send(where, size, src_of, dst, send, recv, order):
    offs, back = offsets(size)
    copies = []
    for j in order:
        copy = ring_copy(
            where, size, offs[j], src_of(j), dst.at[back[j]], send.at[j], recv.at[back[j]]
        )
        copy.start()
        copies.append(copy)
    return copies


def ring_wait(where, size, dst, send, recv, order):
    offs, _ = offsets(size)
    for j in order:
        ring_copy(where, size, offs[j], dst.at[j], dst.at[j], send.at[j], recv.at[j]).wait_recv()


def greet(axes):
    barrier = pltpu.get_barrier_semaphore()
    total = 0
    for axis, size in axes:
        me = lax.axis_index(axis)
        for k in range(1, size):
            pl.semaphore_signal(
                barrier,
                inc=1,
                device_id={axis: lax.rem(me + k, size)},
                device_id_type=MESH,
            )
            total += 1
    return barrier, total


def stack_rows(blocks, stack, count, rows):
    for i in range(count):
        stack[i * rows : (i + 1) * rows, :] = blocks[i].astype(F32)
    return stack[...].astype(BF16)


def added(blocks, count):
    total = blocks[0].astype(F32)
    for i in range(1, count):
        total = total + blocks[i].astype(F32)
    return total


def layer_kernel(
    sizes,
    stop,
    lengths, tokens_in, inverse_in, attn_gain_in, latent_gain_in, post_gain_in, ffn_gain_in,
    out_gain_in, gate_vector_in, routes_in, route_weights_in,
    w_latent, w_rope_key, w_query, w_absorb_key, w_absorb_value, w_out,
    cache_latent, cache_rope,
    w_exp_gate, w_exp_up, w_exp_down, w_dense_gate, w_dense_up, w_dense_down,
    output, latent_out, rope_out,
    tokens, inverse, attn_gain, latent_gain, post_gain, ffn_gain, out_gain, gate_vector,
    routes, route_weights, w_front, w_rope, wk, wv, wo, lat, rop, wg, wu, wd, dg, du, dd,
    hid, stack, qmsg_src, qmsg, fmsg_src, fmsg, wk_pad, q_lat, q_rot, lat_rep, rope_rep,
    gw, ws, gat, stack_x, xs, outs, back_in, part_src, parts,
    in_sem, far_send, far_recv,
    hid_send, hid_recv, q_send, q_recv, f_send, f_recv,
    wv_send, wv_recv, wo_send, wo_recv, fv_send, fv_recv, fo_send, fo_recv,
    gw_send, gw_recv, ws_send, ws_recv, g_send, g_recv, x_send, x_recv,
    o_send, o_recv, p_send, p_recv,
):
    nz, ny, nc, nx = sizes["ep_0"], sizes["ep_1"], sizes["ep_2"], sizes["tp"]
    z, y, core = lax.axis_index("ep_0"), lax.axis_index("ep_1"), lax.axis_index("ep_2")
    x = lax.axis_index("tp")
    rows, width = tokens.shape
    experts = nz * ny * nc
    heads, nope, rank = w_absorb_key.shape
    part = w_latent.shape[0]
    rope = w_rope_key.shape[0]
    span = nope + rope
    barrier, total = greet((("tp", nx), ("ep_2", nc), ("ep_1", ny), ("ep_0", nz)))

    moves = [
        (tokens_in, tokens), (attn_gain_in, attn_gain),
        (routes_in, routes), (route_weights_in, route_weights), (inverse_in, inverse),
    ]
    front = [(w_rope_key, w_rope)]
    for h in range(heads):
        front.append((w_query.at[pl.ds(h * span, nope)], w_front.at[pl.ds(h * nope, nope)]))
    front.append((w_latent, w_front.at[pl.ds(heads * nope, part)]))
    for h in range(heads):
        front.append(
            (
                w_query.at[pl.ds(h * span + nope, rope)],
                w_front.at[pl.ds(heads * nope + part + h * rope, rope)],
            )
        )
    front.append((w_absorb_key, wk))
    middle = [
        (latent_gain_in, latent_gain), (cache_latent, lat), (cache_rope, rop),
        (w_absorb_value, wv.at[x]), (w_out, wo.at[x]), (post_gain_in, post_gain), (ffn_gain_in, ffn_gain),
        (out_gain_in, out_gain), (gate_vector_in, gate_vector),
    ]
    pairs = [
        (w_exp_gate, wg), (w_exp_up, wu), (w_exp_down, wd),
        (w_dense_gate, dg), (w_dense_up, du), (w_dense_down, dd),
    ]
    back = [(src, dst.at[core]) for src, dst in pairs]
    started = []
    for src, dst in moves + front + middle + back:
        copy = pltpu.make_async_copy(src, dst, in_sem.at[len(started)])
        copy.start()
        started.append(copy)
    waiting = iter(started)

    def take(count):
        for _ in range(count):
            next(waiting).wait()

    take(len(moves))
    toks = tokens[...].astype(F32)
    hidden = normalize(toks, attn_gain[...]).astype(BF16)
    hid[x] = hidden
    lane = lax.broadcasted_iota(jnp.int32, (rows, experts), 1)
    chosen = routes[...]
    given = route_weights[...]
    spread = jnp.zeros((rows, experts), F32)
    for k in range(routes.shape[1]):
        spread = spread + jnp.where(lane == chosen[:, k : k + 1], given[:, k : k + 1], 0.0)
    gw[0] = spread

    pl.semaphore_wait(barrier, total)
    sent = []

    def finish():
        for copy in waiting:
            copy.wait()
        for copy in sent:
            copy.wait_send()
        output[...] = toks.astype(BF16)

    sent += exchange("tp", nx, x, lambda p: hid.at[x], hid, hid_send, hid_recv)
    other = lax.rem(core + 1, nc)
    share = heads // nc
    mine = pl.ds(core * share, share)
    theirs = pl.ds(other * share, share)

    def weights_along_x(k):
        partner = lax.rem(x + k, nx)
        for src, dst, send, recv in (
            (w_absorb_value, wv, wv_send, wv_recv), (w_out, wo, wo_send, wo_recv)
        ):
            copy = pltpu.make_async_remote_copy(
                src_ref=src.at[mine], dst_ref=dst.at[x, mine],
                send_sem=send.at[k - 1], recv_sem=recv.at[nx - k - 1],
                device_id={"tp": partner}, device_id_type=MESH,
            )
            copy.start()
            sent.append(copy)

    def passed_on(k, start):
        source = lax.rem(x + k, nx)
        for dst, send, recv, far_send_, far_recv_ in (
            (wv, wv_send, wv_recv, fv_send, fv_recv), (wo, wo_send, wo_recv, fo_send, fo_recv)
        ):
            if start:
                pltpu.make_async_remote_copy(
                    src_ref=dst.at[source, mine], dst_ref=dst.at[source, mine],
                    send_sem=send.at[k - 1], recv_sem=recv.at[k - 1],
                    device_id={"tp": source}, device_id_type=MESH,
                ).wait_recv()
                copy = pltpu.make_async_remote_copy(
                    src_ref=dst.at[source, mine], dst_ref=dst.at[source, mine],
                    send_sem=far_send_.at[k - 1], recv_sem=far_recv_.at[k - 1],
                    device_id={"ep_2": other}, device_id_type=MESH,
                )
                copy.start()
                sent.append(copy)
            else:
                pltpu.make_async_remote_copy(
                    src_ref=dst.at[source, theirs], dst_ref=dst.at[source, theirs],
                    send_sem=far_send_.at[k - 1], recv_sem=far_recv_.at[k - 1],
                    device_id={"ep_2": other}, device_id_type=MESH,
                ).wait_recv()

    near_x = [k for k in range(1, nx) if k in (1, nx - 1)]
    far_x = [k for k in range(1, nx) if k not in near_x]
    for k in near_x:
        weights_along_x(k)
    far = [
        pltpu.make_async_remote_copy(
            src_ref=src, dst_ref=dst.at[core], send_sem=far_send.at[i], recv_sem=far_recv.at[i],
            device_id={"ep_2": other}, device_id_type=MESH,
        )
        for i, (src, dst) in enumerate(pairs)
    ]
    for copy in far:
        copy.start()
    ring = ny
    far_first = list(range(ring - 1, 0, -1))

    def along_a(off):
        return {
            "ep_0": lax.rem(z + core * off + ring, ring),
            "ep_1": lax.rem(y + (1 - core) * off + ring, ring),
        }

    def along_b(off):
        return {
            "ep_0": lax.rem(z + (1 - core) * off + ring, ring),
            "ep_1": lax.rem(y + core * off + ring, ring),
        }

    sent += ring_send(along_a, ring, lambda j: gw.at[0], gw, gw_send, gw_recv, far_first)

    total_heads = nx * heads
    all_rows = total_heads * rows
    row = lax.broadcasted_iota(jnp.int32, (all_rows, rope), 0) % rows
    held = jnp.zeros((all_rows, rope), F32)
    for s in range(rows):
        held = jnp.where(row == s, lengths[s].astype(F32), held)
    angles = held * inverse[...]
    cos = jnp.cos(angles)
    sin = jnp.sin(angles)
    first_half = lax.broadcasted_iota(jnp.int32, (all_rows, rope), 1) < rope // 2
    sin = jnp.where(first_half, -sin, sin)
    wk_pad[...] = jnp.zeros(wk_pad.shape, BF16)
    take(len(front))
    for h in range(heads):
        wk_pad[h * nope : (h + 1) * nope, h * rank : (h + 1) * rank] = wk[h]
    rope_pre = dot_nt(hidden, w_rope[...])
    new_rope = (rope_pre * cos[:rows] + swap_halves(rope_pre) * sin[:rows]).astype(BF16)
    rope_out[...] = new_rope
    arrived("tp", nx, x, hid, hid_send, hid_recv)
    projected = dot_nt(stack_rows(hid, stack, nx, rows), w_front[...])
    flat = heads * nope
    query_latent = dot(projected[:, :flat].astype(BF16), wk_pad[...])
    for t in range(nx):
        for h in range(heads):
            qmsg_src[t, h] = query_latent[
                t * rows : (t + 1) * rows, h * rank : (h + 1) * rank
            ].astype(BF16)
        fmsg_src[t] = projected[t * rows : (t + 1) * rows, flat:]
    sent += exchange("tp", nx, x, lambda p: fmsg_src.at[p], fmsg, f_send, f_recv)
    sent += exchange("tp", nx, x, lambda p: qmsg_src.at[p], qmsg, q_send, q_recv)
    for k in far_x:
        weights_along_x(k)
    qmsg[x] = qmsg_src[x]
    fmsg[x] = fmsg_src[x]
    ring_wait(along_a, ring, gw, gw_send, gw_recv, far_first)
    for i in range(ring):
        ws[0, i * rows : (i + 1) * rows, :] = gw[i]
    arrived("tp", nx, x, fmsg, f_send, f_recv)
    pieces = [fmsg[t] for t in range(nx)]
    latent_full = jnp.concatenate([p[:, :part] for p in pieces], axis=1)
    take(len(middle))
    new_latent = normalize(latent_full, latent_gain[...]).astype(BF16)
    latent_out[...] = new_latent
    latent_f = new_latent.astype(F32)
    rope_f = new_rope.astype(F32)
    for t in range(nx):
        values = pieces[t].astype(BF16).astype(F32)
        for h in range(heads):
            at = (t * heads + h) * rows
            q_rot[at : at + rows, :] = values[:, part + h * rope : part + (h + 1) * rope]
            lat_rep[at : at + rows, :] = latent_f
            rope_rep[at : at + rows, :] = rope_f
    arrived("tp", nx, x, qmsg, q_send, q_recv)
    sent += ring_send(along_b, ring, lambda j: ws.at[0], ws, ws_send, ws_recv, far_first)
    for t in range(nx):
        for h in range(heads):
            at = (t * heads + h) * rows
            q_lat[at : at + rows, :] = qmsg[t, h].astype(F32)
    for k in near_x:
        passed_on(k, True)

    def early():
        for copy in far:
            copy.wait()
        ring_wait(along_b, ring, ws, ws_send, ws_recv, far_first)

    if stop == 2:
        for k in far_x:
            passed_on(k, True)
        for k in near_x + far_x:
            passed_on(k, False)
        early()
        return finish()
    scaling = float(span) ** (-0.5)
    cached = lat.shape[1]
    sequence = lax.broadcasted_iota(jnp.int32, (all_rows, cached), 0) % rows
    position = lax.broadcasted_iota(jnp.int32, (all_rows, cached), 1)
    ql_f = q_lat[...]
    ql = ql_f.astype(BF16)
    raw = q_rot[...]
    qr = (raw * cos + swap_halves(raw) * sin).astype(BF16)
    scores = jnp.zeros((all_rows, cached), F32)
    limit = jnp.zeros((all_rows, cached), jnp.int32)
    for s in range(rows):
        scores = jnp.where(sequence == s, dot_nt(ql, lat[s]) + dot(qr, rop[s]), scores)
        limit = jnp.where(sequence == s, lengths[s], limit)
    own = jnp.sum(ql_f * lat_rep[...], axis=-1, keepdims=True)
    own = (own + jnp.sum(qr.astype(F32) * rope_rep[...], axis=-1, keepdims=True)) * scaling
    scores = jnp.where(position < limit, scores * scaling, negative)
    top = jnp.maximum(jnp.max(scores, axis=-1, keepdims=True), own)
    weights = jnp.exp(scores - top)
    own_weight = jnp.exp(own - top)
    whole = jnp.sum(weights, axis=-1, keepdims=True) + own_weight
    probs = weights / whole
    own_prob = (own_weight / whole).astype(BF16).astype(F32)
    got = own_prob * lat_rep[...]
    for s in range(rows):
        got = got + dot(jnp.where(sequence == s, probs, 0.0).astype(BF16), lat[s])
    attended = got.astype(BF16)
    for k in far_x:
        passed_on(k, True)
    for k in near_x + far_x:
        passed_on(k, False)
    v_head = wv.shape[2]
    heads_out = dot_nt(attended, wv[...].reshape(total_heads * v_head, rank))
    of_row = lax.broadcasted_iota(jnp.int32, heads_out.shape, 0) // rows
    of_column = lax.broadcasted_iota(jnp.int32, heads_out.shape, 1) // v_head
    heads_out = jnp.where(of_row == of_column, heads_out, 0.0)
    head_out = heads_out[:rows]
    for n in range(1, total_heads):
        head_out = head_out + heads_out[n * rows : (n + 1) * rows]
    head_out = head_out.astype(BF16)
    group = heads * v_head
    mixed = jnp.zeros((rows, width), F32)
    for t in range(nx):
        piece = dot(head_out[:, t * group : (t + 1) * group], wo[t].reshape(group, width))
        mixed = mixed + piece.astype(BF16).astype(F32)
    if stop == 4:
        early()
        return finish()
    residual = (toks + normalize(mixed, post_gain[...])).astype(BF16)
    ffn_in = normalize(residual, ffn_gain[...]).astype(BF16)

    gat[0] = ffn_in
    sent += ring_send(along_a, ring, lambda j: gat.at[0], gat, g_send, g_recv, far_first)
    early()
    take(len(back))
    ring_wait(along_a, ring, gat, g_send, g_recv, far_first)
    xs[0] = stack_rows(gat, stack_x, ring, rows)
    sent += ring_send(along_b, ring, lambda j: xs.at[0], xs, x_send, x_recv, far_first)
    if stop == 5:
        ring_wait(along_b, ring, xs, x_send, x_recv, far_first)
        return finish()
    block = ring * rows
    chip = (z * ny + y) * nc
    units = nc * dg.shape[1]
    dense_gate = dg[...].reshape(units, width)
    dense_up = du[...].reshape(units, width)
    dense_down = dd[...].reshape(units, width)
    down = wd[...].reshape(nc * wd.shape[2], width)
    for low, high in groups(ring):
        ring_wait(
            along_b, ring, xs, x_send, x_recv, [j for j in range(high - 1, low - 1, -1) if j]
        )
        count = (high - low) * block
        every = xs[low:high].reshape(count, width)
        spread = ws[low:high].reshape(count, experts)
        columns = lax.broadcasted_iota(jnp.int32, (count, experts), 1)
        acts = []
        for e in range(nc):
            share = jnp.sum(jnp.where(columns == chip + e, spread, 0.0), axis=1, keepdims=True)
            act = silu(dot(every, wg[e, 0])) * dot(every, wu[e, 0])
            acts.append((act * share).astype(BF16))
        gate = jnp.sum(every.astype(F32) * gate_vector[...], axis=1, keepdims=True)
        gate = 1.0 / (1.0 + jnp.exp(-gate))
        dense = silu(dot_nt(every, dense_gate)) * dot_nt(every, dense_up)
        dense = (dense * gate).astype(BF16)
        shares = dot(jnp.concatenate(acts, axis=1), down) + dot(dense, dense_down)
        outs[low:high] = shares.astype(BF16).reshape(high - low, block, width)
        sent += ring_send(
            along_b, ring, lambda j: outs.at[j], back_in, o_send, o_recv,
            [j for j in range(high - 1, low - 1, -1) if j],
        )
    if stop == 6:
        ring_wait(along_b, ring, back_in, o_send, o_recv, far_first)
        return finish()
    whole = outs[0].astype(F32)
    for j in far_first:
        ring_wait(along_b, ring, back_in, o_send, o_recv, [j])
        whole = whole + back_in[j].astype(F32)
    for i in range(ring):
        part_src[i] = whole[i * rows : (i + 1) * rows, :].astype(BF16)
    sent += ring_send(along_a, ring, lambda j: part_src.at[j], parts, p_send, p_recv, far_first)
    combined = part_src[0].astype(F32)
    for j in far_first:
        ring_wait(along_a, ring, parts, p_send, p_recv, [j])
        combined = combined + parts[j].astype(F32)
    output[...] = (residual.astype(F32) + normalize(combined, out_gain[...])).astype(BF16)
    for copy in sent:
        copy.wait_send()


def groups(ring):
    if ring == 8:
        return ((5, 8), (3, 5), (0, 3))
    return ((ring // 2, ring), (0, ring // 2))


def tail_kernel(a, b, c, a_out, b_out, c_out):
    a_out[...] = a[...]
    b_out[...] = b[...]
    c_out[...] = c[...]


def in_vmem(count):
    return [pl.BlockSpec(memory_space=pltpu.VMEM)] * count


def in_place(count):
    return [pl.BlockSpec(memory_space=pl.ANY)] * count


def semaphores(*counts):
    return [pltpu.SemaphoreType.DMA((n,)) for n in counts]


def shards(
    sizes,
    stop,
    tokens,
    lengths,
    cache_latent,
    cache_rope,
    attn_gain,
    latent_gain,
    post_gain,
    ffn_gain,
    out_gain,
    w_latent,
    w_rope_key,
    w_query,
    w_absorb_key,
    w_absorb_value,
    w_out,
    routes,
    route_weights,
    w_exp_gate,
    w_exp_up,
    w_exp_down,
    w_dense_gate,
    w_dense_up,
    w_dense_down,
    dense_gate_vector,
):
    rows, width = tokens.shape
    nz, ny, nc, nx = sizes["ep_0"], sizes["ep_1"], sizes["ep_2"], sizes["tp"]
    experts = nz * ny * nc
    heads, nope, rank = w_absorb_key.shape
    rope = w_rope_key.shape[1]
    part = w_latent.shape[1]
    floats = part + heads * rope
    inverse = np.float32(rope_base) ** (-np.arange(rope // 2, dtype=np.float32) / (rope // 2))
    inverse = np.concatenate([inverse, inverse])[None]
    V = pltpu.VMEM
    weights = (w_exp_gate, w_exp_up, w_exp_down, w_dense_gate, w_dense_up, w_dense_down)
    outs = (
        jax.ShapeDtypeStruct((rows, width), BF16),
        jax.ShapeDtypeStruct((rows, rank), BF16),
        jax.ShapeDtypeStruct((rows, rope), BF16),
    )
    args = (
        lengths, tokens, jnp.asarray(inverse), attn_gain[None], latent_gain[None], post_gain[None],
        ffn_gain[None], out_gain[None], dense_gate_vector[None], routes, route_weights,
        w_latent.T, w_rope_key.T, w_query.T, w_absorb_key, jnp.swapaxes(w_absorb_value, 1, 2),
        w_out.reshape(heads, -1, width), cache_latent, cache_rope, *weights,
    )
    results = pl.pallas_call(
        functools.partial(layer_kernel, sizes, stop),
        out_shape=outs,
        in_specs=[pl.BlockSpec(memory_space=pltpu.SMEM)] + in_place(len(args) - 1),
        out_specs=tuple(in_vmem(3)),
        scratch_shapes=[
            V((rows, width), BF16),
            V((1, rope), F32),
            V((1, width), F32),
            V((1, rank), F32),
            V((1, width), F32),
            V((1, width), F32),
            V((1, width), F32),
            V((1, width), F32),
            V(routes.shape, jnp.int32),
            V(route_weights.shape, F32),
            V((heads * nope + floats, width), BF16),
            V((rope, width), BF16),
            V(w_absorb_key.shape, BF16),
            V((nx, heads, w_absorb_value.shape[2], rank), BF16),
            V((nx, heads, w_absorb_value.shape[2], width), BF16),
            V(cache_latent.shape, BF16),
            V(cache_rope.shape, BF16),
            *[V((nc, *w.shape), BF16) for w in weights],
            V((nx, rows, width), BF16),
            V((nx * rows, width), F32),
            V((nx, heads, rows, rank), BF16),
            V((nx, heads, rows, rank), BF16),
            V((nx, rows, floats), F32),
            V((nx, rows, floats), F32),
            V((heads * nope, heads * rank), BF16),
            V((nx * heads * rows, rank), F32),
            V((nx * heads * rows, rope), F32),
            V((nx * heads * rows, rank), F32),
            V((nx * heads * rows, rope), F32),
            V((ny, rows, experts), F32),
            V((ny, ny * rows, experts), F32),
            V((ny, rows, width), BF16),
            V((ny * rows, width), F32),
            V((ny, ny * rows, width), BF16),
            V((ny, ny * rows, width), BF16),
            V((ny, ny * rows, width), BF16),
            V((ny, rows, width), BF16),
            V((ny, rows, width), BF16),
        ]
        + semaphores(40, 6, 6, *([nx - 1, nx] * 3), *([nx - 1] * 8), *([ny] * 12)),
        compiler_params=pltpu.CompilerParams(collective_id=0, has_side_effects=True),
        name="layer",
    )(*args)
    return pl.pallas_call(
        tail_kernel,
        out_shape=outs,
        in_specs=in_vmem(3),
        out_specs=tuple(in_vmem(3)),
        name="tail",
    )(*results)


def solution(mesh, dims=(8, 8, 2), stop=0):
    torus = Mesh(mesh.devices.reshape(*dims, mesh.shape["tp"]), EP_TP)
    placed = (
        P(EP_TP, None),
        P(EP_TP),
        P(EP_TP, None, None),
        P(EP_TP, None, None),
        P(),
        P(),
        P(),
        P(),
        P(),
        P(None, "tp"),
        P(),
        P(None, "tp"),
        P("tp", None, None),
        P("tp", None, None),
        P("tp", None),
        P(EP_TP, None),
        P(EP_TP, None),
        P(EP, None, None),
        P(EP, None, None),
        P(EP, None, None),
        P(EP, None),
        P(EP, None),
        P(EP, None),
        P(),
    )
    return jax.shard_map(
        functools.partial(shards, dict(torus.shape), stop),
        mesh=torus,
        in_specs=placed,
        out_specs=(P(EP_TP, None), P(EP_TP, None), P(EP_TP, None)),
        check_vma=False,
    )
```

```python
import functools

import jax
import jax.numpy as jnp
import numpy as np
from jax import lax
from jax.experimental import pallas as pl
from jax.experimental.pallas import tpu as pltpu
from jax.sharding import Mesh
from jax.sharding import PartitionSpec as P

EP = ("ep_0", "ep_1", "ep_2")
EP_TP = ("ep_0", "ep_1", "ep_2", "tp")
MESH = pl.DeviceIdType.MESH
F32 = jnp.float32
BF16 = jnp.bfloat16

epsilon = 1e-06
rope_base = 10000.0
negative = -1e30


def dot(a, b):
    return jnp.dot(a, b, preferred_element_type=F32)


def dot_nt(a, b):
    return lax.dot_general(a, b, (((1,), (1,)), ((), ())), preferred_element_type=F32)


def normalize(values, gain):
    values = values.astype(F32)
    mean = jnp.mean(values * values, axis=-1, keepdims=True)
    return values * lax.rsqrt(mean + epsilon) * gain


def swap_halves(values):
    half = values.shape[-1] // 2
    return jnp.concatenate([values[:, half:], values[:, :half]], axis=1)


def silu(values):
    return values / (1.0 + jnp.exp(-values))


def exchange(axis, size, me, src_of, dst, send, recv):
    copies = []
    for k in range(1, size):
        partner = lax.rem(me + k, size)
        copy = pltpu.make_async_remote_copy(
            src_ref=src_of(partner),
            dst_ref=dst.at[me],
            send_sem=send.at[k - 1],
            recv_sem=recv.at[me],
            device_id={axis: partner},
            device_id_type=MESH,
        )
        copy.start()
        copies.append(copy)
    return copies


def arrived(axis, size, me, dst, send, recv):
    for k in range(1, size):
        partner = lax.rem(me + k, size)
        pltpu.make_async_remote_copy(
            src_ref=dst.at[partner],
            dst_ref=dst.at[partner],
            send_sem=send.at[k - 1],
            recv_sem=recv.at[partner],
            device_id={axis: partner},
            device_id_type=MESH,
        ).wait_recv()


def offsets(size):
    order = [0]
    for k in range(1, (size + 1) // 2):
        order += [k, -k]
    if size % 2 == 0:
        order.append(size // 2)
    return order, [order.index(-k if -k in order else k) for k in order]


def ring_copy(where, size, off, src, dst, send, recv):
    return pltpu.make_async_remote_copy(
        src_ref=src, dst_ref=dst, send_sem=send, recv_sem=recv,
        device_id=where(off), device_id_type=MESH,
    )


def ring_send(where, size, src_of, dst, send, recv, order):
    offs, back = offsets(size)
    copies = []
    for j in order:
        copy = ring_copy(
            where, size, offs[j], src_of(j), dst.at[back[j]], send.at[j], recv.at[back[j]]
        )
        copy.start()
        copies.append(copy)
    return copies


def ring_wait(where, size, dst, send, recv, order):
    offs, _ = offsets(size)
    for j in order:
        ring_copy(where, size, offs[j], dst.at[j], dst.at[j], send.at[j], recv.at[j]).wait_recv()


def tell(semaphore, axes):
    total = 0
    for axis, distances in axes:
        me = lax.axis_index(axis)
        for k in distances:
            pl.semaphore_signal(
                semaphore,
                inc=1,
                device_id={axis: lax.rem(me + k, lax.axis_size(axis))},
                device_id_type=MESH,
            )
            total += 1
    return total


def greet(axes):
    barrier = pltpu.get_barrier_semaphore()
    return barrier, tell(barrier, axes)


def stack_rows(blocks, stack, count, rows):
    for i in range(count):
        stack[i * rows : (i + 1) * rows, :] = blocks[i].astype(F32)
    return stack[...].astype(BF16)


def added(blocks, count):
    total = blocks[0].astype(F32)
    for i in range(1, count):
        total = total + blocks[i].astype(F32)
    return total


def layer_kernel(
    sizes,
    stop,
    lengths_in, tokens_in, inverse_in, attn_gain_in, latent_gain_in, post_gain_in, ffn_gain_in,
    out_gain_in, gate_vector_in, routes_in, route_weights_in,
    w_latent, w_rope_key, w_query, w_absorb_key, w_absorb_value, w_out,
    cache_latent, cache_rope,
    w_exp_gate, w_exp_up, w_exp_down, w_dense_gate, w_dense_up, w_dense_down,
    output, latent_out, rope_out,
    lengths, tokens, inverse, attn_gain, latent_gain, post_gain, ffn_gain, out_gain, gate_vector,
    routes, route_weights, w_front, w_rope, wk, wv, wo, lat, rop, wg, wu, wd, dg, du, dd,
    hid, stack, qmsg_src, qmsg, fmsg_src, fmsg, wk_pad, q_lat, q_rot, lat_rep, rope_rep,
    gw, ws, gat, stack_x, xs, outs, back_in, part_src, parts,
    second_sem, fourth_sem, in_sem, far_send, far_recv,
    hid_send, hid_recv, q_send, q_recv, f_send, f_recv,
    wv_send, wv_recv, wo_send, wo_recv, fv_send, fv_recv, fo_send, fo_recv,
    gw_send, gw_recv, ws_send, ws_recv, g_send, g_recv, x_send, x_recv,
    o_send, o_recv, p_send, p_recv,
):
    nz, ny, nc, nx = sizes["ep_0"], sizes["ep_1"], sizes["ep_2"], sizes["tp"]
    z, y, core = lax.axis_index("ep_0"), lax.axis_index("ep_1"), lax.axis_index("ep_2")
    x = lax.axis_index("tp")
    rows, width = tokens.shape
    experts = nz * ny * nc
    heads, nope, rank = w_absorb_key.shape
    part = w_latent.shape[0]
    rope = w_rope_key.shape[0]
    span = nope + rope
    ring = ny
    chained = ring == 8
    met = (1, ring - 1) if chained else tuple(range(1, ring))
    barrier, total = greet((("tp", range(1, nx)), ("ep_2", range(1, nc)), ("ep_1", met), ("ep_0", met)))

    moves = [
        (lengths_in, lengths), (tokens_in, tokens), (attn_gain_in, attn_gain),
        (routes_in, routes), (route_weights_in, route_weights), (inverse_in, inverse),
    ]
    front = [(w_rope_key, w_rope)]
    for h in range(heads):
        front.append((w_query.at[pl.ds(h * span, nope)], w_front.at[pl.ds(h * nope, nope)]))
    front.append((w_latent, w_front.at[pl.ds(heads * nope, part)]))
    for h in range(heads):
        front.append(
            (
                w_query.at[pl.ds(h * span + nope, rope)],
                w_front.at[pl.ds(heads * nope + part + h * rope, rope)],
            )
        )
    front.append((w_absorb_key, wk))
    middle = [
        (latent_gain_in, latent_gain), (cache_latent, lat), (cache_rope, rop),
        (w_absorb_value, wv.at[x]), (w_out, wo.at[x]), (post_gain_in, post_gain), (ffn_gain_in, ffn_gain),
        (out_gain_in, out_gain), (gate_vector_in, gate_vector),
    ]
    pairs = [
        (w_exp_gate, wg), (w_exp_up, wu), (w_exp_down, wd),
        (w_dense_gate, dg), (w_dense_up, du), (w_dense_down, dd),
    ]
    back = [(src, dst.at[core]) for src, dst in pairs]
    started = []
    for src, dst in moves + front + middle + back:
        copy = pltpu.make_async_copy(src, dst, in_sem.at[len(started)])
        copy.start()
        started.append(copy)
    waiting = iter(started)

    def take(count):
        for _ in range(count):
            next(waiting).wait()

    take(len(moves))
    toks = tokens[...].astype(F32)
    hidden = normalize(toks, attn_gain[...]).astype(BF16)
    hid[x] = hidden
    lane = lax.broadcasted_iota(jnp.int32, (rows, experts), 1)
    chosen = routes[...]
    given = route_weights[...]
    spread = jnp.zeros((rows, experts), F32)
    for k in range(routes.shape[1]):
        spread = spread + jnp.where(lane == chosen[:, k : k + 1], given[:, k : k + 1], 0.0)
    gw[0] = spread

    pl.semaphore_wait(barrier, total)
    if chained:
        heard = tell(second_sem, (("ep_1", met), ("ep_0", met)))
    sent = []

    def finish():
        for copy in waiting:
            copy.wait()
        for copy in sent:
            copy.wait_send()
        output[...] = toks.astype(BF16)

    sent += exchange("tp", nx, x, lambda p: hid.at[x], hid, hid_send, hid_recv)
    other = lax.rem(core + 1, nc)
    share = heads // nc
    mine = pl.ds(core * share, share)
    theirs = pl.ds(other * share, share)

    def weights_along_x(k):
        partner = lax.rem(x + k, nx)
        for src, dst, send, recv in (
            (w_absorb_value, wv, wv_send, wv_recv), (w_out, wo, wo_send, wo_recv)
        ):
            copy = pltpu.make_async_remote_copy(
                src_ref=src.at[mine], dst_ref=dst.at[x, mine],
                send_sem=send.at[k - 1], recv_sem=recv.at[nx - k - 1],
                device_id={"tp": partner}, device_id_type=MESH,
            )
            copy.start()
            sent.append(copy)

    def passed_on(k, start):
        source = lax.rem(x + k, nx)
        for dst, send, recv, far_send_, far_recv_ in (
            (wv, wv_send, wv_recv, fv_send, fv_recv), (wo, wo_send, wo_recv, fo_send, fo_recv)
        ):
            if start:
                pltpu.make_async_remote_copy(
                    src_ref=dst.at[source, mine], dst_ref=dst.at[source, mine],
                    send_sem=send.at[k - 1], recv_sem=recv.at[k - 1],
                    device_id={"tp": source}, device_id_type=MESH,
                ).wait_recv()
                copy = pltpu.make_async_remote_copy(
                    src_ref=dst.at[source, mine], dst_ref=dst.at[source, mine],
                    send_sem=far_send_.at[k - 1], recv_sem=far_recv_.at[k - 1],
                    device_id={"ep_2": other}, device_id_type=MESH,
                )
                copy.start()
                sent.append(copy)
            else:
                pltpu.make_async_remote_copy(
                    src_ref=dst.at[source, theirs], dst_ref=dst.at[source, theirs],
                    send_sem=far_send_.at[k - 1], recv_sem=far_recv_.at[k - 1],
                    device_id={"ep_2": other}, device_id_type=MESH,
                ).wait_recv()

    near_x = [k for k in range(1, nx) if k in (1, nx - 1)]
    far_x = [k for k in range(1, nx) if k not in near_x]
    for k in near_x:
        weights_along_x(k)
    far = [
        pltpu.make_async_remote_copy(
            src_ref=src, dst_ref=dst.at[core], send_sem=far_send.at[i], recv_sem=far_recv.at[i],
            device_id={"ep_2": other}, device_id_type=MESH,
        )
        for i, (src, dst) in enumerate(pairs)
    ]
    for copy in far:
        copy.start()
    far_first = list(range(ring - 1, 0, -1))

    def along_a(off):
        return {
            "ep_0": lax.rem(z + core * off + ring, ring),
            "ep_1": lax.rem(y + (1 - core) * off + ring, ring),
        }

    def along_b(off):
        return {
            "ep_0": lax.rem(z + (1 - core) * off + ring, ring),
            "ep_1": lax.rem(y + core * off + ring, ring),
        }


    total_heads = nx * heads
    all_rows = total_heads * rows
    row = lax.broadcasted_iota(jnp.int32, (all_rows, rope), 0) % rows
    held = jnp.zeros((all_rows, rope), F32)
    for s in range(rows):
        held = jnp.where(row == s, lengths[s].astype(F32), held)
    angles = held * inverse[...]
    cos = jnp.cos(angles)
    sin = jnp.sin(angles)
    first_half = lax.broadcasted_iota(jnp.int32, (all_rows, rope), 1) < rope // 2
    sin = jnp.where(first_half, -sin, sin)
    wk_pad[...] = jnp.zeros(wk_pad.shape, BF16)
    take(len(front))
    for h in range(heads):
        wk_pad[h * nope : (h + 1) * nope, h * rank : (h + 1) * rank] = wk[h]
    rope_pre = dot_nt(hidden, w_rope[...])
    new_rope = (rope_pre * cos[:rows] + swap_halves(rope_pre) * sin[:rows]).astype(BF16)
    rope_out[...] = new_rope
    if chained:
        pl.semaphore_wait(second_sem, heard)
        heard = tell(fourth_sem, (("ep_1", (2, 6)), ("ep_0", (2, 6))))
    arrived("tp", nx, x, hid, hid_send, hid_recv)
    projected = dot_nt(stack_rows(hid, stack, nx, rows), w_front[...])
    flat = heads * nope
    query_latent = dot(projected[:, :flat].astype(BF16), wk_pad[...])
    for t in range(nx):
        for h in range(heads):
            qmsg_src[t, h] = query_latent[
                t * rows : (t + 1) * rows, h * rank : (h + 1) * rank
            ].astype(BF16)
        fmsg_src[t] = projected[t * rows : (t + 1) * rows, flat:]
    sent += exchange("tp", nx, x, lambda p: fmsg_src.at[p], fmsg, f_send, f_recv)
    sent += exchange("tp", nx, x, lambda p: qmsg_src.at[p], qmsg, q_send, q_recv)
    for k in far_x:
        weights_along_x(k)
    qmsg[x] = qmsg_src[x]
    fmsg[x] = fmsg_src[x]
    if chained:
        pl.semaphore_wait(fourth_sem, heard)
    sent += ring_send(along_a, ring, lambda j: gw.at[0], gw, gw_send, gw_recv, far_first)
    arrived("tp", nx, x, fmsg, f_send, f_recv)
    pieces = [fmsg[t] for t in range(nx)]
    latent_full = jnp.concatenate([p[:, :part] for p in pieces], axis=1)
    take(len(middle))
    new_latent = normalize(latent_full, latent_gain[...]).astype(BF16)
    latent_out[...] = new_latent
    latent_f = new_latent.astype(F32)
    rope_f = new_rope.astype(F32)
    for t in range(nx):
        values = pieces[t].astype(BF16).astype(F32)
        for h in range(heads):
            at = (t * heads + h) * rows
            q_rot[at : at + rows, :] = values[:, part + h * rope : part + (h + 1) * rope]
            lat_rep[at : at + rows, :] = latent_f
            rope_rep[at : at + rows, :] = rope_f
    arrived("tp", nx, x, qmsg, q_send, q_recv)
    for t in range(nx):
        for h in range(heads):
            at = (t * heads + h) * rows
            q_lat[at : at + rows, :] = qmsg[t, h].astype(F32)
    for k in near_x:
        passed_on(k, True)

    def early():
        for copy in far:
            copy.wait()
        ring_wait(along_b, ring, ws, ws_send, ws_recv, far_first)

    scaling = float(span) ** (-0.5)
    cached = lat.shape[1]
    sequence = lax.broadcasted_iota(jnp.int32, (all_rows, cached), 0) % rows
    position = lax.broadcasted_iota(jnp.int32, (all_rows, cached), 1)
    ql_f = q_lat[...]
    ql = ql_f.astype(BF16)
    raw = q_rot[...]
    qr = (raw * cos + swap_halves(raw) * sin).astype(BF16)
    scores = jnp.zeros((all_rows, cached), F32)
    limit = jnp.zeros((all_rows, cached), jnp.int32)
    for s in range(rows):
        scores = jnp.where(sequence == s, dot_nt(ql, lat[s]) + dot(qr, rop[s]), scores)
        limit = jnp.where(sequence == s, lengths[s], limit)
    own = jnp.sum(ql_f * lat_rep[...], axis=-1, keepdims=True)
    own = (own + jnp.sum(qr.astype(F32) * rope_rep[...], axis=-1, keepdims=True)) * scaling
    scores = jnp.where(position < limit, scores * scaling, negative)
    top = jnp.maximum(jnp.max(scores, axis=-1, keepdims=True), own)
    weights = jnp.exp(scores - top)
    own_weight = jnp.exp(own - top)
    whole = jnp.sum(weights, axis=-1, keepdims=True) + own_weight
    probs = weights / whole
    own_prob = (own_weight / whole).astype(BF16).astype(F32)
    got = own_prob * lat_rep[...]
    for s in range(rows):
        got = got + dot(jnp.where(sequence == s, probs, 0.0).astype(BF16), lat[s])
    attended = got.astype(BF16)
    ring_wait(along_a, ring, gw, gw_send, gw_recv, far_first)
    for i in range(ring):
        ws[0, i * rows : (i + 1) * rows, :] = gw[i]
    sent += ring_send(along_b, ring, lambda j: ws.at[0], ws, ws_send, ws_recv, far_first)
    for k in far_x:
        passed_on(k, True)
    for k in near_x + far_x:
        passed_on(k, False)
    v_head = wv.shape[2]
    heads_out = dot_nt(attended, wv[...].reshape(total_heads * v_head, rank))
    of_row = lax.broadcasted_iota(jnp.int32, heads_out.shape, 0) // rows
    of_column = lax.broadcasted_iota(jnp.int32, heads_out.shape, 1) // v_head
    heads_out = jnp.where(of_row == of_column, heads_out, 0.0)
    head_out = heads_out[:rows]
    for n in range(1, total_heads):
        head_out = head_out + heads_out[n * rows : (n + 1) * rows]
    head_out = head_out.astype(BF16)
    group = heads * v_head
    mixed = jnp.zeros((rows, width), F32)
    for t in range(nx):
        piece = dot(head_out[:, t * group : (t + 1) * group], wo[t].reshape(group, width))
        mixed = mixed + piece.astype(BF16).astype(F32)
    if stop == 4:
        early()
        return finish()
    residual = (toks + normalize(mixed, post_gain[...])).astype(BF16)
    ffn_in = normalize(residual, ffn_gain[...]).astype(BF16)

    gat[0] = ffn_in
    sent += ring_send(along_a, ring, lambda j: gat.at[0], gat, g_send, g_recv, far_first)
    early()
    take(len(back))
    ring_wait(along_a, ring, gat, g_send, g_recv, far_first)
    xs[0] = stack_rows(gat, stack_x, ring, rows)
    sent += ring_send(along_b, ring, lambda j: xs.at[0], xs, x_send, x_recv, far_first)
    if stop == 5:
        ring_wait(along_b, ring, xs, x_send, x_recv, far_first)
        return finish()
    block = ring * rows
    chip = (z * ny + y) * nc
    units = nc * dg.shape[1]
    dense_gate = dg[...].reshape(units, width)
    dense_up = du[...].reshape(units, width)
    dense_down = dd[...].reshape(units, width)
    down = wd[...].reshape(nc * wd.shape[2], width)
    for low, high in groups(ring):
        ring_wait(
            along_b, ring, xs, x_send, x_recv, [j for j in range(high - 1, low - 1, -1) if j]
        )
        count = (high - low) * block
        every = xs[low:high].reshape(count, width)
        spread = ws[low:high].reshape(count, experts)
        columns = lax.broadcasted_iota(jnp.int32, (count, experts), 1)
        acts = []
        for e in range(nc):
            share = jnp.sum(jnp.where(columns == chip + e, spread, 0.0), axis=1, keepdims=True)
            act = silu(dot(every, wg[e, 0])) * dot(every, wu[e, 0])
            acts.append((act * share).astype(BF16))
        gate = jnp.sum(every.astype(F32) * gate_vector[...], axis=1, keepdims=True)
        gate = 1.0 / (1.0 + jnp.exp(-gate))
        dense = silu(dot_nt(every, dense_gate)) * dot_nt(every, dense_up)
        dense = (dense * gate).astype(BF16)
        shares = dot(jnp.concatenate(acts, axis=1), down) + dot(dense, dense_down)
        outs[low:high] = shares.astype(BF16).reshape(high - low, block, width)
        sent += ring_send(
            along_b, ring, lambda j: outs.at[j], back_in, o_send, o_recv,
            [j for j in range(high - 1, low - 1, -1) if j],
        )
    if stop == 6:
        ring_wait(along_b, ring, back_in, o_send, o_recv, far_first)
        return finish()
    whole = outs[0].astype(F32)
    for j in far_first:
        ring_wait(along_b, ring, back_in, o_send, o_recv, [j])
        whole = whole + back_in[j].astype(F32)
    for i in range(ring):
        part_src[i] = whole[i * rows : (i + 1) * rows, :].astype(BF16)
    sent += ring_send(along_a, ring, lambda j: part_src.at[j], parts, p_send, p_recv, far_first)
    combined = part_src[0].astype(F32)
    for j in far_first:
        ring_wait(along_a, ring, parts, p_send, p_recv, [j])
        combined = combined + parts[j].astype(F32)
    output[...] = (residual.astype(F32) + normalize(combined, out_gain[...])).astype(BF16)
    for copy in sent:
        copy.wait_send()


def groups(ring):
    if ring == 8:
        return ((0, 1), (7, 8), (5, 7), (3, 5), (1, 3))
    return ((ring // 2, ring), (0, ring // 2))


def tail_kernel(a, b, c, a_out, b_out, c_out):
    a_out[...] = a[...]
    b_out[...] = b[...]
    c_out[...] = c[...]


def in_vmem(count):
    return [pl.BlockSpec(memory_space=pltpu.VMEM)] * count


def in_place(count):
    return [pl.BlockSpec(memory_space=pl.ANY)] * count


def semaphores(*counts):
    return [pltpu.SemaphoreType.DMA((n,)) for n in counts]


def shards(
    sizes,
    stop,
    tokens,
    lengths,
    cache_latent,
    cache_rope,
    attn_gain,
    latent_gain,
    post_gain,
    ffn_gain,
    out_gain,
    w_latent,
    w_rope_key,
    w_query,
    w_absorb_key,
    w_absorb_value,
    w_out,
    routes,
    route_weights,
    w_exp_gate,
    w_exp_up,
    w_exp_down,
    w_dense_gate,
    w_dense_up,
    w_dense_down,
    dense_gate_vector,
):
    rows, width = tokens.shape
    nz, ny, nc, nx = sizes["ep_0"], sizes["ep_1"], sizes["ep_2"], sizes["tp"]
    experts = nz * ny * nc
    heads, nope, rank = w_absorb_key.shape
    rope = w_rope_key.shape[1]
    part = w_latent.shape[1]
    floats = part + heads * rope
    inverse = np.float32(rope_base) ** (-np.arange(rope // 2, dtype=np.float32) / (rope // 2))
    inverse = np.concatenate([inverse, inverse])[None]
    V = pltpu.VMEM
    weights = (w_exp_gate, w_exp_up, w_exp_down, w_dense_gate, w_dense_up, w_dense_down)
    outs = (
        jax.ShapeDtypeStruct((rows, width), BF16),
        jax.ShapeDtypeStruct((rows, rank), BF16),
        jax.ShapeDtypeStruct((rows, rope), BF16),
    )
    args = (
        lengths, tokens, jnp.asarray(inverse), attn_gain[None], latent_gain[None], post_gain[None],
        ffn_gain[None], out_gain[None], dense_gate_vector[None], routes, route_weights,
        w_latent.T, w_rope_key.T, w_query.T, w_absorb_key, jnp.swapaxes(w_absorb_value, 1, 2),
        w_out.reshape(heads, -1, width), cache_latent, cache_rope, *weights,
    )
    results = pl.pallas_call(
        functools.partial(layer_kernel, sizes, stop),
        out_shape=outs,
        in_specs=in_place(len(args)),
        out_specs=tuple(in_vmem(3)),
        scratch_shapes=[
            pltpu.SMEM(lengths.shape, jnp.int32),
            V((rows, width), BF16),
            V((1, rope), F32),
            V((1, width), F32),
            V((1, rank), F32),
            V((1, width), F32),
            V((1, width), F32),
            V((1, width), F32),
            V((1, width), F32),
            V(routes.shape, jnp.int32),
            V(route_weights.shape, F32),
            V((heads * nope + floats, width), BF16),
            V((rope, width), BF16),
            V(w_absorb_key.shape, BF16),
            V((nx, heads, w_absorb_value.shape[2], rank), BF16),
            V((nx, heads, w_absorb_value.shape[2], width), BF16),
            V(cache_latent.shape, BF16),
            V(cache_rope.shape, BF16),
            *[V((nc, *w.shape), BF16) for w in weights],
            V((nx, rows, width), BF16),
            V((nx * rows, width), F32),
            V((nx, heads, rows, rank), BF16),
            V((nx, heads, rows, rank), BF16),
            V((nx, rows, floats), F32),
            V((nx, rows, floats), F32),
            V((heads * nope, heads * rank), BF16),
            V((nx * heads * rows, rank), F32),
            V((nx * heads * rows, rope), F32),
            V((nx * heads * rows, rank), F32),
            V((nx * heads * rows, rope), F32),
            V((ny, rows, experts), F32),
            V((ny, ny * rows, experts), F32),
            V((ny, rows, width), BF16),
            V((ny * rows, width), F32),
            V((ny, ny * rows, width), BF16),
            V((ny, ny * rows, width), BF16),
            V((ny, ny * rows, width), BF16),
            V((ny, rows, width), BF16),
            V((ny, rows, width), BF16),
        ]
        + [pltpu.SemaphoreType.REGULAR] * 2
        + semaphores(40, 6, 6, *([nx - 1, nx] * 3), *([nx - 1] * 8), *([ny] * 12)),
        compiler_params=pltpu.CompilerParams(collective_id=0, has_side_effects=True),
        name="layer",
    )(*args)
    return pl.pallas_call(
        tail_kernel,
        out_shape=outs,
        in_specs=in_vmem(3),
        out_specs=tuple(in_vmem(3)),
        name="tail",
    )(*results)


def solution(mesh, dims=(8, 8, 2), stop=0):
    torus = Mesh(mesh.devices.reshape(*dims, mesh.shape["tp"]), EP_TP)
    placed = (
        P(EP_TP, None),
        P(EP_TP),
        P(EP_TP, None, None),
        P(EP_TP, None, None),
        P(),
        P(),
        P(),
        P(),
        P(),
        P(None, "tp"),
        P(),
        P(None, "tp"),
        P("tp", None, None),
        P("tp", None, None),
        P("tp", None),
        P(EP_TP, None),
        P(EP_TP, None),
        P(EP, None, None),
        P(EP, None, None),
        P(EP, None, None),
        P(EP, None),
        P(EP, None),
        P(EP, None),
        P(),
    )
    return jax.shard_map(
        functools.partial(shards, dict(torus.shape), stop),
        mesh=torus,
        in_specs=placed,
        out_specs=(P(EP_TP, None), P(EP_TP, None), P(EP_TP, None)),
        check_vma=False,
    )
```

```python
import functools

import jax
import jax.numpy as jnp
import numpy as np
from jax import lax
from jax.experimental import pallas as pl
from jax.experimental.pallas import tpu as pltpu
from jax.sharding import Mesh
from jax.sharding import PartitionSpec as P

EP = ("ep_0", "ep_1", "ep_2")
EP_TP = ("ep_0", "ep_1", "ep_2", "tp")
MESH = pl.DeviceIdType.MESH
F32 = jnp.float32
BF16 = jnp.bfloat16

epsilon = 1e-06
rope_base = 10000.0
negative = -1e30


def dot(a, b):
    return jnp.dot(a, b, preferred_element_type=F32)


def dot_nt(a, b):
    return lax.dot_general(a, b, (((1,), (1,)), ((), ())), preferred_element_type=F32)


def normalize(values, gain):
    values = values.astype(F32)
    mean = jnp.mean(values * values, axis=-1, keepdims=True)
    return values * lax.rsqrt(mean + epsilon) * gain


def swap_halves(values):
    half = values.shape[-1] // 2
    return jnp.concatenate([values[:, half:], values[:, :half]], axis=1)


def silu(values):
    return values / (1.0 + jnp.exp(-values))


def exchange(axis, size, me, src_of, dst, send, recv):
    copies = []
    for k in range(1, size):
        partner = lax.rem(me + k, size)
        copy = pltpu.make_async_remote_copy(
            src_ref=src_of(partner),
            dst_ref=dst.at[me],
            send_sem=send.at[k - 1],
            recv_sem=recv.at[me],
            device_id={axis: partner},
            device_id_type=MESH,
        )
        copy.start()
        copies.append(copy)
    return copies


def arrived(axis, size, me, dst, send, recv):
    for k in range(1, size):
        partner = lax.rem(me + k, size)
        pltpu.make_async_remote_copy(
            src_ref=dst.at[partner],
            dst_ref=dst.at[partner],
            send_sem=send.at[k - 1],
            recv_sem=recv.at[partner],
            device_id={axis: partner},
            device_id_type=MESH,
        ).wait_recv()


def offsets(size):
    order = [0]
    for k in range(1, (size + 1) // 2):
        order += [k, -k]
    if size % 2 == 0:
        order.append(size // 2)
    return order, [order.index(-k if -k in order else k) for k in order]


def ring_copy(where, size, off, src, dst, send, recv):
    return pltpu.make_async_remote_copy(
        src_ref=src, dst_ref=dst, send_sem=send, recv_sem=recv,
        device_id=where(off), device_id_type=MESH,
    )


def ring_send(where, size, src_of, dst, send, recv, order):
    offs, back = offsets(size)
    copies = []
    for j in order:
        copy = ring_copy(
            where, size, offs[j], src_of(j), dst.at[back[j]], send.at[j], recv.at[back[j]]
        )
        copy.start()
        copies.append(copy)
    return copies


def ring_wait(where, size, dst, send, recv, order):
    offs, _ = offsets(size)
    for j in order:
        ring_copy(where, size, offs[j], dst.at[j], dst.at[j], send.at[j], recv.at[j]).wait_recv()


def tell(semaphore, axes):
    total = 0
    for axis, distances in axes:
        me = lax.axis_index(axis)
        for k in distances:
            pl.semaphore_signal(
                semaphore,
                inc=1,
                device_id={axis: lax.rem(me + k, lax.axis_size(axis))},
                device_id_type=MESH,
            )
            total += 1
    return total


def greet(axes):
    barrier = pltpu.get_barrier_semaphore()
    return barrier, tell(barrier, axes)


def stack_rows(blocks, stack, count, rows):
    for i in range(count):
        stack[i * rows : (i + 1) * rows, :] = blocks[i].astype(F32)
    return stack[...].astype(BF16)


def added(blocks, count):
    total = blocks[0].astype(F32)
    for i in range(1, count):
        total = total + blocks[i].astype(F32)
    return total


def layer_kernel(
    sizes,
    stop,
    lengths_in, tokens_in, inverse_in, attn_gain_in, latent_gain_in, post_gain_in, ffn_gain_in,
    out_gain_in, gate_vector_in, routes_in, route_weights_in,
    w_latent, w_rope_key, w_query, w_absorb_key, w_absorb_value, w_out,
    cache_latent, cache_rope,
    w_exp_gate, w_exp_up, w_exp_down, w_dense_gate, w_dense_up, w_dense_down,
    output, latent_out, rope_out,
    lengths, tokens, inverse, attn_gain, latent_gain, post_gain, ffn_gain, out_gain, gate_vector,
    routes, route_weights, w_front, w_rope, wk, wv, wo, lat, rop, wg, wu, wd, dg, du, dd,
    hid, stack, qmsg_src, qmsg, fmsg_src, fmsg, wk_pad, q_lat, q_rot, lat_rep, rope_rep,
    gw, ws, gat, stack_x, xs, outs, back_in, part_src, parts,
    second_sem, fourth_sem, in_sem, far_send, far_recv,
    hid_send, hid_recv, q_send, q_recv, f_send, f_recv,
    wv_send, wv_recv, wo_send, wo_recv, fv_send, fv_recv, fo_send, fo_recv,
    gw_send, gw_recv, ws_send, ws_recv, g_send, g_recv, x_send, x_recv,
    o_send, o_recv, p_send, p_recv,
):
    nz, ny, nc, nx = sizes["ep_0"], sizes["ep_1"], sizes["ep_2"], sizes["tp"]
    z, y, core = lax.axis_index("ep_0"), lax.axis_index("ep_1"), lax.axis_index("ep_2")
    x = lax.axis_index("tp")
    rows, width = tokens.shape
    experts = nz * ny * nc
    heads, nope, rank = w_absorb_key.shape
    part = w_latent.shape[0]
    rope = w_rope_key.shape[0]
    span = nope + rope
    ring = ny
    chained = ring == 8
    met = (1, ring - 1) if chained else tuple(range(1, ring))
    barrier, total = greet((("tp", range(1, nx)), ("ep_2", range(1, nc)), ("ep_1", met), ("ep_0", met)))

    moves = [
        (lengths_in, lengths), (tokens_in, tokens), (attn_gain_in, attn_gain),
        (routes_in, routes), (route_weights_in, route_weights), (inverse_in, inverse),
    ]
    front = [(w_rope_key, w_rope)]
    for h in range(heads):
        front.append((w_query.at[pl.ds(h * span, nope)], w_front.at[pl.ds(h * nope, nope)]))
    front.append((w_latent, w_front.at[pl.ds(heads * nope, part)]))
    for h in range(heads):
        front.append(
            (
                w_query.at[pl.ds(h * span + nope, rope)],
                w_front.at[pl.ds(heads * nope + part + h * rope, rope)],
            )
        )
    front.append((w_absorb_key, wk))
    middle = [
        (latent_gain_in, latent_gain), (cache_latent, lat), (cache_rope, rop),
        (w_absorb_value, wv.at[x]), (w_out, wo.at[x]), (post_gain_in, post_gain), (ffn_gain_in, ffn_gain),
        (out_gain_in, out_gain), (gate_vector_in, gate_vector),
    ]
    pairs = [
        (w_exp_gate, wg), (w_exp_up, wu), (w_exp_down, wd),
        (w_dense_gate, dg), (w_dense_up, du), (w_dense_down, dd),
    ]
    back = [(src, dst.at[core]) for src, dst in pairs]
    started = []
    for src, dst in moves + front + middle + back:
        copy = pltpu.make_async_copy(src, dst, in_sem.at[len(started)])
        copy.start()
        started.append(copy)
    waiting = iter(started)

    def take(count):
        for _ in range(count):
            next(waiting).wait()

    take(len(moves))
    toks = tokens[...].astype(F32)
    hidden = normalize(toks, attn_gain[...]).astype(BF16)
    hid[x] = hidden
    lane = lax.broadcasted_iota(jnp.int32, (rows, experts), 1)
    chosen = routes[...]
    given = route_weights[...]
    spread = jnp.zeros((rows, experts), F32)
    for k in range(routes.shape[1]):
        spread = spread + jnp.where(lane == chosen[:, k : k + 1], given[:, k : k + 1], 0.0)
    gw[0] = spread

    pl.semaphore_wait(barrier, total)
    if chained:
        heard = tell(second_sem, (("ep_1", met), ("ep_0", met)))
    sent = []

    def finish():
        for copy in waiting:
            copy.wait()
        for copy in sent:
            copy.wait_send()
        output[...] = toks.astype(BF16)

    sent += exchange("tp", nx, x, lambda p: hid.at[x], hid, hid_send, hid_recv)
    other = lax.rem(core + 1, nc)
    share = heads // nc
    mine = pl.ds(core * share, share)
    theirs = pl.ds(other * share, share)

    def weights_along_x(k):
        partner = lax.rem(x + k, nx)
        for src, dst, send, recv in (
            (w_absorb_value, wv, wv_send, wv_recv), (w_out, wo, wo_send, wo_recv)
        ):
            copy = pltpu.make_async_remote_copy(
                src_ref=src.at[mine], dst_ref=dst.at[x, mine],
                send_sem=send.at[k - 1], recv_sem=recv.at[nx - k - 1],
                device_id={"tp": partner}, device_id_type=MESH,
            )
            copy.start()
            sent.append(copy)

    def passed_on(k, start):
        source = lax.rem(x + k, nx)
        for dst, send, recv, far_send_, far_recv_ in (
            (wv, wv_send, wv_recv, fv_send, fv_recv), (wo, wo_send, wo_recv, fo_send, fo_recv)
        ):
            if start:
                pltpu.make_async_remote_copy(
                    src_ref=dst.at[source, mine], dst_ref=dst.at[source, mine],
                    send_sem=send.at[k - 1], recv_sem=recv.at[k - 1],
                    device_id={"tp": source}, device_id_type=MESH,
                ).wait_recv()
                copy = pltpu.make_async_remote_copy(
                    src_ref=dst.at[source, mine], dst_ref=dst.at[source, mine],
                    send_sem=far_send_.at[k - 1], recv_sem=far_recv_.at[k - 1],
                    device_id={"ep_2": other}, device_id_type=MESH,
                )
                copy.start()
                sent.append(copy)
            else:
                pltpu.make_async_remote_copy(
                    src_ref=dst.at[source, theirs], dst_ref=dst.at[source, theirs],
                    send_sem=far_send_.at[k - 1], recv_sem=far_recv_.at[k - 1],
                    device_id={"ep_2": other}, device_id_type=MESH,
                ).wait_recv()

    near_x = [k for k in range(1, nx) if k in (1, nx - 1)]
    far_x = [k for k in range(1, nx) if k not in near_x]
    for k in near_x:
        weights_along_x(k)
    far = [
        pltpu.make_async_remote_copy(
            src_ref=src, dst_ref=dst.at[core], send_sem=far_send.at[i], recv_sem=far_recv.at[i],
            device_id={"ep_2": other}, device_id_type=MESH,
        )
        for i, (src, dst) in enumerate(pairs)
    ]
    for copy in far:
        copy.start()
    far_first = list(range(ring - 1, 0, -1))

    def along_b(off):
        return {
            "ep_0": lax.rem(z + core * off + ring, ring),
            "ep_1": lax.rem(y + (1 - core) * off + ring, ring),
        }

    def along_a(off):
        return {
            "ep_0": lax.rem(z + (1 - core) * off + ring, ring),
            "ep_1": lax.rem(y + core * off + ring, ring),
        }


    total_heads = nx * heads
    all_rows = total_heads * rows
    row = lax.broadcasted_iota(jnp.int32, (all_rows, rope), 0) % rows
    held = jnp.zeros((all_rows, rope), F32)
    for s in range(rows):
        held = jnp.where(row == s, lengths[s].astype(F32), held)
    angles = held * inverse[...]
    cos = jnp.cos(angles)
    sin = jnp.sin(angles)
    first_half = lax.broadcasted_iota(jnp.int32, (all_rows, rope), 1) < rope // 2
    sin = jnp.where(first_half, -sin, sin)
    wk_pad[...] = jnp.zeros(wk_pad.shape, BF16)
    take(len(front))
    for h in range(heads):
        wk_pad[h * nope : (h + 1) * nope, h * rank : (h + 1) * rank] = wk[h]
    rope_pre = dot_nt(hidden, w_rope[...])
    new_rope = (rope_pre * cos[:rows] + swap_halves(rope_pre) * sin[:rows]).astype(BF16)
    rope_out[...] = new_rope
    if chained:
        pl.semaphore_wait(second_sem, heard)
        heard = tell(fourth_sem, (("ep_1", (2, 6)), ("ep_0", (2, 6))))
    arrived("tp", nx, x, hid, hid_send, hid_recv)
    projected = dot_nt(stack_rows(hid, stack, nx, rows), w_front[...])
    flat = heads * nope
    query_latent = dot(projected[:, :flat].astype(BF16), wk_pad[...])
    for t in range(nx):
        for h in range(heads):
            qmsg_src[t, h] = query_latent[
                t * rows : (t + 1) * rows, h * rank : (h + 1) * rank
            ].astype(BF16)
        fmsg_src[t] = projected[t * rows : (t + 1) * rows, flat:]
    sent += exchange("tp", nx, x, lambda p: fmsg_src.at[p], fmsg, f_send, f_recv)
    sent += exchange("tp", nx, x, lambda p: qmsg_src.at[p], qmsg, q_send, q_recv)
    for k in far_x:
        weights_along_x(k)
    qmsg[x] = qmsg_src[x]
    fmsg[x] = fmsg_src[x]
    if chained:
        pl.semaphore_wait(fourth_sem, heard)
    sent += ring_send(along_a, ring, lambda j: gw.at[0], gw, gw_send, gw_recv, far_first)
    arrived("tp", nx, x, fmsg, f_send, f_recv)
    pieces = [fmsg[t] for t in range(nx)]
    latent_full = jnp.concatenate([p[:, :part] for p in pieces], axis=1)
    take(len(middle))
    new_latent = normalize(latent_full, latent_gain[...]).astype(BF16)
    latent_out[...] = new_latent
    latent_f = new_latent.astype(F32)
    rope_f = new_rope.astype(F32)
    for t in range(nx):
        values = pieces[t].astype(BF16).astype(F32)
        for h in range(heads):
            at = (t * heads + h) * rows
            q_rot[at : at + rows, :] = values[:, part + h * rope : part + (h + 1) * rope]
            lat_rep[at : at + rows, :] = latent_f
            rope_rep[at : at + rows, :] = rope_f
    arrived("tp", nx, x, qmsg, q_send, q_recv)
    for t in range(nx):
        for h in range(heads):
            at = (t * heads + h) * rows
            q_lat[at : at + rows, :] = qmsg[t, h].astype(F32)
    for k in near_x:
        passed_on(k, True)

    def early():
        for copy in far:
            copy.wait()
        ring_wait(along_b, ring, ws, ws_send, ws_recv, far_first)

    scaling = float(span) ** (-0.5)
    cached = lat.shape[1]
    sequence = lax.broadcasted_iota(jnp.int32, (all_rows, cached), 0) % rows
    position = lax.broadcasted_iota(jnp.int32, (all_rows, cached), 1)
    ql_f = q_lat[...]
    ql = ql_f.astype(BF16)
    raw = q_rot[...]
    qr = (raw * cos + swap_halves(raw) * sin).astype(BF16)
    scores = jnp.zeros((all_rows, cached), F32)
    limit = jnp.zeros((all_rows, cached), jnp.int32)
    for s in range(rows):
        scores = jnp.where(sequence == s, dot_nt(ql, lat[s]) + dot(qr, rop[s]), scores)
        limit = jnp.where(sequence == s, lengths[s], limit)
    own = jnp.sum(ql_f * lat_rep[...], axis=-1, keepdims=True)
    own = (own + jnp.sum(qr.astype(F32) * rope_rep[...], axis=-1, keepdims=True)) * scaling
    scores = jnp.where(position < limit, scores * scaling, negative)
    top = jnp.maximum(jnp.max(scores, axis=-1, keepdims=True), own)
    weights = jnp.exp(scores - top)
    own_weight = jnp.exp(own - top)
    whole = jnp.sum(weights, axis=-1, keepdims=True) + own_weight
    probs = weights / whole
    own_prob = (own_weight / whole).astype(BF16).astype(F32)
    got = own_prob * lat_rep[...]
    for s in range(rows):
        got = got + dot(jnp.where(sequence == s, probs, 0.0).astype(BF16), lat[s])
    attended = got.astype(BF16)
    ring_wait(along_a, ring, gw, gw_send, gw_recv, far_first)
    for i in range(ring):
        ws[0, i * rows : (i + 1) * rows, :] = gw[i]
    sent += ring_send(along_b, ring, lambda j: ws.at[0], ws, ws_send, ws_recv, far_first)
    for k in far_x:
        passed_on(k, True)
    for k in near_x + far_x:
        passed_on(k, False)
    v_head = wv.shape[2]
    heads_out = dot_nt(attended, wv[...].reshape(total_heads * v_head, rank))
    of_row = lax.broadcasted_iota(jnp.int32, heads_out.shape, 0) // rows
    of_column = lax.broadcasted_iota(jnp.int32, heads_out.shape, 1) // v_head
    heads_out = jnp.where(of_row == of_column, heads_out, 0.0)
    head_out = heads_out[:rows]
    for n in range(1, total_heads):
        head_out = head_out + heads_out[n * rows : (n + 1) * rows]
    head_out = head_out.astype(BF16)
    group = heads * v_head
    mixed = jnp.zeros((rows, width), F32)
    for t in range(nx):
        piece = dot(head_out[:, t * group : (t + 1) * group], wo[t].reshape(group, width))
        mixed = mixed + piece.astype(BF16).astype(F32)
    if stop == 4:
        early()
        return finish()
    residual = (toks + normalize(mixed, post_gain[...])).astype(BF16)
    ffn_in = normalize(residual, ffn_gain[...]).astype(BF16)

    gat[0] = ffn_in
    sent += ring_send(along_a, ring, lambda j: gat.at[0], gat, g_send, g_recv, far_first)
    early()
    take(len(back))
    ring_wait(along_a, ring, gat, g_send, g_recv, far_first)
    xs[0] = stack_rows(gat, stack_x, ring, rows)
    sent += ring_send(along_b, ring, lambda j: xs.at[0], xs, x_send, x_recv, far_first)
    if stop == 5:
        ring_wait(along_b, ring, xs, x_send, x_recv, far_first)
        return finish()
    block = ring * rows
    chip = (z * ny + y) * nc
    units = nc * dg.shape[1]
    dense_gate = dg[...].reshape(units, width)
    dense_up = du[...].reshape(units, width)
    dense_down = dd[...].reshape(units, width)
    down = wd[...].reshape(nc * wd.shape[2], width)
    for low, high in groups(ring):
        ring_wait(
            along_b, ring, xs, x_send, x_recv, [j for j in range(high - 1, low - 1, -1) if j]
        )
        count = (high - low) * block
        every = xs[low:high].reshape(count, width)
        spread = ws[low:high].reshape(count, experts)
        columns = lax.broadcasted_iota(jnp.int32, (count, experts), 1)
        acts = []
        for e in range(nc):
            share = jnp.sum(jnp.where(columns == chip + e, spread, 0.0), axis=1, keepdims=True)
            act = silu(dot(every, wg[e, 0])) * dot(every, wu[e, 0])
            acts.append((act * share).astype(BF16))
        gate = jnp.sum(every.astype(F32) * gate_vector[...], axis=1, keepdims=True)
        gate = 1.0 / (1.0 + jnp.exp(-gate))
        dense = silu(dot_nt(every, dense_gate)) * dot_nt(every, dense_up)
        dense = (dense * gate).astype(BF16)
        shares = dot(jnp.concatenate(acts, axis=1), down) + dot(dense, dense_down)
        outs[low:high] = shares.astype(BF16).reshape(high - low, block, width)
        sent += ring_send(
            along_b, ring, lambda j: outs.at[j], back_in, o_send, o_recv,
            [j for j in range(high - 1, low - 1, -1) if j],
        )
    if stop == 6:
        ring_wait(along_b, ring, back_in, o_send, o_recv, far_first)
        return finish()
    whole = outs[0].astype(F32)
    for j in far_first:
        ring_wait(along_b, ring, back_in, o_send, o_recv, [j])
        whole = whole + back_in[j].astype(F32)
    for i in range(ring):
        part_src[i] = whole[i * rows : (i + 1) * rows, :].astype(BF16)
    sent += ring_send(along_a, ring, lambda j: part_src.at[j], parts, p_send, p_recv, far_first)
    combined = part_src[0].astype(F32)
    for j in far_first:
        ring_wait(along_a, ring, parts, p_send, p_recv, [j])
        combined = combined + parts[j].astype(F32)
    output[...] = (residual.astype(F32) + normalize(combined, out_gain[...])).astype(BF16)
    for copy in sent:
        copy.wait_send()


def groups(ring):
    if ring == 8:
        return ((0, 1), (7, 8), (5, 7), (3, 5), (1, 3))
    return ((ring // 2, ring), (0, ring // 2))


def tail_kernel(a, b, c, a_out, b_out, c_out):
    a_out[...] = a[...]
    b_out[...] = b[...]
    c_out[...] = c[...]


def in_vmem(count):
    return [pl.BlockSpec(memory_space=pltpu.VMEM)] * count


def in_place(count):
    return [pl.BlockSpec(memory_space=pl.ANY)] * count


def semaphores(*counts):
    return [pltpu.SemaphoreType.DMA((n,)) for n in counts]


def shards(
    sizes,
    stop,
    tokens,
    lengths,
    cache_latent,
    cache_rope,
    attn_gain,
    latent_gain,
    post_gain,
    ffn_gain,
    out_gain,
    w_latent,
    w_rope_key,
    w_query,
    w_absorb_key,
    w_absorb_value,
    w_out,
    routes,
    route_weights,
    w_exp_gate,
    w_exp_up,
    w_exp_down,
    w_dense_gate,
    w_dense_up,
    w_dense_down,
    dense_gate_vector,
):
    rows, width = tokens.shape
    nz, ny, nc, nx = sizes["ep_0"], sizes["ep_1"], sizes["ep_2"], sizes["tp"]
    experts = nz * ny * nc
    heads, nope, rank = w_absorb_key.shape
    rope = w_rope_key.shape[1]
    part = w_latent.shape[1]
    floats = part + heads * rope
    inverse = np.float32(rope_base) ** (-np.arange(rope // 2, dtype=np.float32) / (rope // 2))
    inverse = np.concatenate([inverse, inverse])[None]
    V = pltpu.VMEM
    weights = (w_exp_gate, w_exp_up, w_exp_down, w_dense_gate, w_dense_up, w_dense_down)
    outs = (
        jax.ShapeDtypeStruct((rows, width), BF16),
        jax.ShapeDtypeStruct((rows, rank), BF16),
        jax.ShapeDtypeStruct((rows, rope), BF16),
    )
    args = (
        lengths, tokens, jnp.asarray(inverse), attn_gain[None], latent_gain[None], post_gain[None],
        ffn_gain[None], out_gain[None], dense_gate_vector[None], routes, route_weights,
        w_latent.T, w_rope_key.T, w_query.T, w_absorb_key, jnp.swapaxes(w_absorb_value, 1, 2),
        w_out.reshape(heads, -1, width), cache_latent, cache_rope, *weights,
    )
    results = pl.pallas_call(
        functools.partial(layer_kernel, sizes, stop),
        out_shape=tuple(V(o.shape, o.dtype) for o in outs),
        in_specs=in_place(len(args)),
        out_specs=tuple(in_vmem(3)),
        scratch_shapes=[
            pltpu.SMEM(lengths.shape, jnp.int32),
            V((rows, width), BF16),
            V((1, rope), F32),
            V((1, width), F32),
            V((1, rank), F32),
            V((1, width), F32),
            V((1, width), F32),
            V((1, width), F32),
            V((1, width), F32),
            V(routes.shape, jnp.int32),
            V(route_weights.shape, F32),
            V((heads * nope + floats, width), BF16),
            V((rope, width), BF16),
            V(w_absorb_key.shape, BF16),
            V((nx, heads, w_absorb_value.shape[2], rank), BF16),
            V((nx, heads, w_absorb_value.shape[2], width), BF16),
            V(cache_latent.shape, BF16),
            V(cache_rope.shape, BF16),
            *[V((nc, *w.shape), BF16) for w in weights],
            V((nx, rows, width), BF16),
            V((nx * rows, width), F32),
            V((nx, heads, rows, rank), BF16),
            V((nx, heads, rows, rank), BF16),
            V((nx, rows, floats), F32),
            V((nx, rows, floats), F32),
            V((heads * nope, heads * rank), BF16),
            V((nx * heads * rows, rank), F32),
            V((nx * heads * rows, rope), F32),
            V((nx * heads * rows, rank), F32),
            V((nx * heads * rows, rope), F32),
            V((ny, rows, experts), F32),
            V((ny, ny * rows, experts), F32),
            V((ny, rows, width), BF16),
            V((ny * rows, width), F32),
            V((ny, ny * rows, width), BF16),
            V((ny, ny * rows, width), BF16),
            V((ny, ny * rows, width), BF16),
            V((ny, rows, width), BF16),
            V((ny, rows, width), BF16),
        ]
        + [pltpu.SemaphoreType.REGULAR] * 2
        + semaphores(40, 6, 6, *([nx - 1, nx] * 3), *([nx - 1] * 8), *([ny] * 12)),
        compiler_params=pltpu.CompilerParams(collective_id=0, has_side_effects=True),
        name="layer",
    )(*args)
    return pl.pallas_call(
        tail_kernel,
        out_shape=outs,
        in_specs=in_vmem(3),
        out_specs=tuple(in_vmem(3)),
        name="tail",
    )(*[pltpu.with_memory_space_constraint(r, pltpu.VMEM) for r in results])


def solution(mesh, dims=(8, 8, 2), stop=0):
    torus = Mesh(mesh.devices.reshape(*dims, mesh.shape["tp"]), EP_TP)
    placed = (
        P(EP_TP, None),
        P(EP_TP),
        P(EP_TP, None, None),
        P(EP_TP, None, None),
        P(),
        P(),
        P(),
        P(),
        P(),
        P(None, "tp"),
        P(),
        P(None, "tp"),
        P("tp", None, None),
        P("tp", None, None),
        P("tp", None),
        P(EP_TP, None),
        P(EP_TP, None),
        P(EP, None, None),
        P(EP, None, None),
        P(EP, None, None),
        P(EP, None),
        P(EP, None),
        P(EP, None),
        P(),
    )
    return jax.shard_map(
        functools.partial(shards, dict(torus.shape), stop),
        mesh=torus,
        in_specs=placed,
        out_specs=(P(EP_TP, None), P(EP_TP, None), P(EP_TP, None)),
        check_vma=False,
    )
```

```python
import functools

import jax
import jax.numpy as jnp
import numpy as np
from jax import lax
from jax.experimental import pallas as pl
from jax.experimental.pallas import tpu as pltpu
from jax.sharding import Mesh
from jax.sharding import PartitionSpec as P

EP = ("ep_0", "ep_1", "ep_2")
EP_TP = ("ep_0", "ep_1", "ep_2", "tp")
MESH = pl.DeviceIdType.MESH
F32 = jnp.float32
BF16 = jnp.bfloat16

epsilon = 1e-06
rope_base = 10000.0
negative = -1e30


def dot(a, b):
    return jnp.dot(a, b, preferred_element_type=F32)


def dot_nt(a, b):
    return lax.dot_general(a, b, (((1,), (1,)), ((), ())), preferred_element_type=F32)


def normalize(values, gain):
    values = values.astype(F32)
    mean = jnp.mean(values * values, axis=-1, keepdims=True)
    return values * lax.rsqrt(mean + epsilon) * gain


def swap_halves(values):
    half = values.shape[-1] // 2
    return jnp.concatenate([values[:, half:], values[:, :half]], axis=1)


def silu(values):
    return values / (1.0 + jnp.exp(-values))


def exchange(axis, size, me, src_of, dst, send, recv):
    copies = []
    for k in range(1, size):
        partner = lax.rem(me + k, size)
        copy = pltpu.make_async_remote_copy(
            src_ref=src_of(partner),
            dst_ref=dst.at[me],
            send_sem=send.at[k - 1],
            recv_sem=recv.at[me],
            device_id={axis: partner},
            device_id_type=MESH,
        )
        copy.start()
        copies.append(copy)
    return copies


def arrived(axis, size, me, dst, send, recv):
    for k in range(1, size):
        partner = lax.rem(me + k, size)
        pltpu.make_async_remote_copy(
            src_ref=dst.at[partner],
            dst_ref=dst.at[partner],
            send_sem=send.at[k - 1],
            recv_sem=recv.at[partner],
            device_id={axis: partner},
            device_id_type=MESH,
        ).wait_recv()


def offsets(size):
    order = [0]
    for k in range(1, (size + 1) // 2):
        order += [k, -k]
    if size % 2 == 0:
        order.append(size // 2)
    return order, [order.index(-k if -k in order else k) for k in order]


def ring_copy(where, size, off, src, dst, send, recv):
    return pltpu.make_async_remote_copy(
        src_ref=src, dst_ref=dst, send_sem=send, recv_sem=recv,
        device_id=where(off), device_id_type=MESH,
    )


def ring_send(where, size, src_of, dst, send, recv, order):
    offs, back = offsets(size)
    copies = []
    for j in order:
        copy = ring_copy(
            where, size, offs[j], src_of(j), dst.at[back[j]], send.at[j], recv.at[back[j]]
        )
        copy.start()
        copies.append(copy)
    return copies


def ring_wait(where, size, dst, send, recv, order):
    offs, _ = offsets(size)
    for j in order:
        ring_copy(where, size, offs[j], dst.at[j], dst.at[j], send.at[j], recv.at[j]).wait_recv()


def tell(semaphore, axes):
    total = 0
    for axis, distances in axes:
        me = lax.axis_index(axis)
        for k in distances:
            pl.semaphore_signal(
                semaphore,
                inc=1,
                device_id={axis: lax.rem(me + k, lax.axis_size(axis))},
                device_id_type=MESH,
            )
            total += 1
    return total


def greet(axes):
    barrier = pltpu.get_barrier_semaphore()
    return barrier, tell(barrier, axes)


def stack_rows(blocks, stack, count, rows):
    for i in range(count):
        stack[i * rows : (i + 1) * rows, :] = blocks[i].astype(F32)
    return stack[...].astype(BF16)


def added(blocks, count):
    total = blocks[0].astype(F32)
    for i in range(1, count):
        total = total + blocks[i].astype(F32)
    return total


def layer_kernel(
    sizes,
    stop,
    lengths_in, tokens_in, inverse_in, attn_gain_in, latent_gain_in, post_gain_in, ffn_gain_in,
    out_gain_in, gate_vector_in, routes_in, route_weights_in,
    w_latent, w_rope_key, w_query, w_absorb_key, w_absorb_value, w_out,
    cache_latent, cache_rope,
    w_exp_gate, w_exp_up, w_exp_down, w_dense_gate, w_dense_up, w_dense_down,
    output, latent_out, rope_out,
    lengths, tokens, inverse, attn_gain, latent_gain, post_gain, ffn_gain, out_gain, gate_vector,
    routes, route_weights, w_front, w_rope, wk, wv, wo, lat, rop, wg, wu, wd, dg, du, dd,
    hid, stack, qmsg_src, qmsg, fmsg_src, fmsg, wk_pad, q_lat, q_rot, lat_rep, rope_rep,
    gw, ws, gat, stack_x, xs, outs, back_in, part_src, parts,
    second_sem, fourth_sem, in_sem, far_send, far_recv,
    hid_send, hid_recv, q_send, q_recv, f_send, f_recv,
    wv_send, wv_recv, wo_send, wo_recv, fv_send, fv_recv, fo_send, fo_recv,
    gw_send, gw_recv, ws_send, ws_recv, g_send, g_recv, x_send, x_recv,
    o_send, o_recv, p_send, p_recv,
):
    nz, ny, nc, nx = sizes["ep_0"], sizes["ep_1"], sizes["ep_2"], sizes["tp"]
    z, y, core = lax.axis_index("ep_0"), lax.axis_index("ep_1"), lax.axis_index("ep_2")
    x = lax.axis_index("tp")
    rows, width = tokens.shape
    experts = nz * ny * nc
    heads, nope, rank = w_absorb_key.shape
    part = w_latent.shape[0]
    rope = w_rope_key.shape[0]
    span = nope + rope
    ring = ny
    chained = ring == 8
    met = (1, ring - 1) if chained else tuple(range(1, ring))
    barrier, total = greet((("tp", range(1, nx)), ("ep_2", range(1, nc)), ("ep_1", met), ("ep_0", met)))

    moves = [
        (lengths_in, lengths), (tokens_in, tokens), (attn_gain_in, attn_gain),
        (routes_in, routes), (route_weights_in, route_weights), (inverse_in, inverse),
    ]
    front = [(w_rope_key, w_rope)]
    for h in range(heads):
        front.append((w_query.at[pl.ds(h * span, nope)], w_front.at[pl.ds(h * nope, nope)]))
    front.append((w_latent, w_front.at[pl.ds(heads * nope, part)]))
    for h in range(heads):
        front.append(
            (
                w_query.at[pl.ds(h * span + nope, rope)],
                w_front.at[pl.ds(heads * nope + part + h * rope, rope)],
            )
        )
    front.append((w_absorb_key, wk))
    middle = [
        (latent_gain_in, latent_gain), (cache_latent, lat), (cache_rope, rop),
        (w_absorb_value, wv.at[x]), (w_out, wo.at[x]), (post_gain_in, post_gain), (ffn_gain_in, ffn_gain),
        (out_gain_in, out_gain), (gate_vector_in, gate_vector),
    ]
    pairs = [
        (w_exp_gate, wg), (w_exp_up, wu), (w_exp_down, wd),
        (w_dense_gate, dg), (w_dense_up, du), (w_dense_down, dd),
    ]
    back = [(src, dst.at[core]) for src, dst in pairs]
    started = []
    for src, dst in moves + front + middle + back:
        copy = pltpu.make_async_copy(src, dst, in_sem.at[len(started)])
        copy.start()
        started.append(copy)
    waiting = iter(started)

    def take(count):
        for _ in range(count):
            next(waiting).wait()

    take(len(moves))
    toks = tokens[...].astype(F32)
    hidden = normalize(toks, attn_gain[...]).astype(BF16)
    hid[x] = hidden
    lane = lax.broadcasted_iota(jnp.int32, (rows, experts), 1)
    chosen = routes[...]
    given = route_weights[...]
    spread = jnp.zeros((rows, experts), F32)
    for k in range(routes.shape[1]):
        spread = spread + jnp.where(lane == chosen[:, k : k + 1], given[:, k : k + 1], 0.0)
    gw[0] = spread

    pl.semaphore_wait(barrier, total)
    if chained:
        heard = tell(second_sem, (("ep_1", met), ("ep_0", met)))
    sent = []

    def finish():
        for copy in waiting:
            copy.wait()
        for copy in sent:
            copy.wait_send()
        output[...] = toks.astype(BF16)

    sent += exchange("tp", nx, x, lambda p: hid.at[x], hid, hid_send, hid_recv)
    other = lax.rem(core + 1, nc)
    share = heads // nc
    mine = pl.ds(core * share, share)
    theirs = pl.ds(other * share, share)

    def weights_along_x(k):
        partner = lax.rem(x + k, nx)
        for src, dst, send, recv in (
            (w_absorb_value, wv, wv_send, wv_recv), (w_out, wo, wo_send, wo_recv)
        ):
            copy = pltpu.make_async_remote_copy(
                src_ref=src.at[mine], dst_ref=dst.at[x, mine],
                send_sem=send.at[k - 1], recv_sem=recv.at[nx - k - 1],
                device_id={"tp": partner}, device_id_type=MESH,
            )
            copy.start()
            sent.append(copy)

    def passed_on(k, start):
        source = lax.rem(x + k, nx)
        for dst, send, recv, far_send_, far_recv_ in (
            (wv, wv_send, wv_recv, fv_send, fv_recv), (wo, wo_send, wo_recv, fo_send, fo_recv)
        ):
            if start:
                pltpu.make_async_remote_copy(
                    src_ref=dst.at[source, mine], dst_ref=dst.at[source, mine],
                    send_sem=send.at[k - 1], recv_sem=recv.at[k - 1],
                    device_id={"tp": source}, device_id_type=MESH,
                ).wait_recv()
                copy = pltpu.make_async_remote_copy(
                    src_ref=dst.at[source, mine], dst_ref=dst.at[source, mine],
                    send_sem=far_send_.at[k - 1], recv_sem=far_recv_.at[k - 1],
                    device_id={"ep_2": other}, device_id_type=MESH,
                )
                copy.start()
                sent.append(copy)
            else:
                pltpu.make_async_remote_copy(
                    src_ref=dst.at[source, theirs], dst_ref=dst.at[source, theirs],
                    send_sem=far_send_.at[k - 1], recv_sem=far_recv_.at[k - 1],
                    device_id={"ep_2": other}, device_id_type=MESH,
                ).wait_recv()

    near_x = [k for k in range(1, nx) if k in (1, nx - 1)]
    far_x = [k for k in range(1, nx) if k not in near_x]
    for k in near_x:
        weights_along_x(k)
    far = [
        pltpu.make_async_remote_copy(
            src_ref=src, dst_ref=dst.at[core], send_sem=far_send.at[i], recv_sem=far_recv.at[i],
            device_id={"ep_2": other}, device_id_type=MESH,
        )
        for i, (src, dst) in enumerate(pairs)
    ]
    for copy in far:
        copy.start()
    far_first = list(range(ring - 1, 0, -1))

    def along_b(off):
        return {
            "ep_0": lax.rem(z + core * off + ring, ring),
            "ep_1": lax.rem(y + (1 - core) * off + ring, ring),
        }

    def along_a(off):
        return {
            "ep_0": lax.rem(z + (1 - core) * off + ring, ring),
            "ep_1": lax.rem(y + core * off + ring, ring),
        }


    total_heads = nx * heads
    all_rows = total_heads * rows
    row = lax.broadcasted_iota(jnp.int32, (all_rows, rope), 0) % rows
    held = jnp.zeros((all_rows, rope), F32)
    for s in range(rows):
        held = jnp.where(row == s, lengths[s].astype(F32), held)
    angles = held * inverse[...]
    cos = jnp.cos(angles)
    sin = jnp.sin(angles)
    first_half = lax.broadcasted_iota(jnp.int32, (all_rows, rope), 1) < rope // 2
    sin = jnp.where(first_half, -sin, sin)
    wk_pad[...] = jnp.zeros(wk_pad.shape, BF16)
    take(len(front))
    for h in range(heads):
        wk_pad[h * nope : (h + 1) * nope, h * rank : (h + 1) * rank] = wk[h]
    rope_pre = dot_nt(hidden, w_rope[...])
    new_rope = (rope_pre * cos[:rows] + swap_halves(rope_pre) * sin[:rows]).astype(BF16)
    rope_out[...] = new_rope
    if chained:
        pl.semaphore_wait(second_sem, heard)
        heard = tell(fourth_sem, (("ep_1", (2, 6)), ("ep_0", (2, 6))))
    arrived("tp", nx, x, hid, hid_send, hid_recv)
    projected = dot_nt(stack_rows(hid, stack, nx, rows), w_front[...])
    flat = heads * nope
    query_latent = dot(projected[:, :flat].astype(BF16), wk_pad[...])
    for t in range(nx):
        for h in range(heads):
            qmsg_src[t, h] = query_latent[
                t * rows : (t + 1) * rows, h * rank : (h + 1) * rank
            ].astype(BF16)
        fmsg_src[t] = projected[t * rows : (t + 1) * rows, flat:]
    sent += exchange("tp", nx, x, lambda p: fmsg_src.at[p], fmsg, f_send, f_recv)
    sent += exchange("tp", nx, x, lambda p: qmsg_src.at[p], qmsg, q_send, q_recv)
    for k in far_x:
        weights_along_x(k)
    qmsg[x] = qmsg_src[x]
    fmsg[x] = fmsg_src[x]
    if chained:
        pl.semaphore_wait(fourth_sem, heard)
    sent += ring_send(along_a, ring, lambda j: gw.at[0], gw, gw_send, gw_recv, far_first)
    arrived("tp", nx, x, fmsg, f_send, f_recv)
    pieces = [fmsg[t] for t in range(nx)]
    latent_full = jnp.concatenate([p[:, :part] for p in pieces], axis=1)
    take(len(middle))
    new_latent = normalize(latent_full, latent_gain[...]).astype(BF16)
    latent_out[...] = new_latent
    latent_f = new_latent.astype(F32)
    rope_f = new_rope.astype(F32)
    for t in range(nx):
        values = pieces[t].astype(BF16).astype(F32)
        for h in range(heads):
            at = (t * heads + h) * rows
            q_rot[at : at + rows, :] = values[:, part + h * rope : part + (h + 1) * rope]
            lat_rep[at : at + rows, :] = latent_f
            rope_rep[at : at + rows, :] = rope_f
    arrived("tp", nx, x, qmsg, q_send, q_recv)
    for t in range(nx):
        for h in range(heads):
            at = (t * heads + h) * rows
            q_lat[at : at + rows, :] = qmsg[t, h].astype(F32)
    for k in near_x:
        passed_on(k, True)

    def early():
        for copy in far:
            copy.wait()
        ring_wait(along_b, ring, ws, ws_send, ws_recv, far_first)

    scaling = float(span) ** (-0.5)
    cached = lat.shape[1]
    sequence = lax.broadcasted_iota(jnp.int32, (all_rows, cached), 0) % rows
    position = lax.broadcasted_iota(jnp.int32, (all_rows, cached), 1)
    ql_f = q_lat[...]
    ql = ql_f.astype(BF16)
    raw = q_rot[...]
    qr = (raw * cos + swap_halves(raw) * sin).astype(BF16)
    scores = jnp.zeros((all_rows, cached), F32)
    limit = jnp.zeros((all_rows, cached), jnp.int32)
    for s in range(rows):
        scores = jnp.where(sequence == s, dot_nt(ql, lat[s]) + dot(qr, rop[s]), scores)
        limit = jnp.where(sequence == s, lengths[s], limit)
    own = jnp.sum(ql_f * lat_rep[...], axis=-1, keepdims=True)
    own = (own + jnp.sum(qr.astype(F32) * rope_rep[...], axis=-1, keepdims=True)) * scaling
    scores = jnp.where(position < limit, scores * scaling, negative)
    top = jnp.maximum(jnp.max(scores, axis=-1, keepdims=True), own)
    weights = jnp.exp(scores - top)
    own_weight = jnp.exp(own - top)
    whole = jnp.sum(weights, axis=-1, keepdims=True) + own_weight
    probs = weights / whole
    own_prob = (own_weight / whole).astype(BF16).astype(F32)
    got = own_prob * lat_rep[...]
    for s in range(rows):
        got = got + dot(jnp.where(sequence == s, probs, 0.0).astype(BF16), lat[s])
    attended = got.astype(BF16)
    for k in far_x:
        passed_on(k, True)
    for k in near_x + far_x:
        passed_on(k, False)
    v_head = wv.shape[2]
    heads_out = dot_nt(attended, wv[...].reshape(total_heads * v_head, rank))
    of_row = lax.broadcasted_iota(jnp.int32, heads_out.shape, 0) // rows
    of_column = lax.broadcasted_iota(jnp.int32, heads_out.shape, 1) // v_head
    heads_out = jnp.where(of_row == of_column, heads_out, 0.0)
    head_out = heads_out[:rows]
    for n in range(1, total_heads):
        head_out = head_out + heads_out[n * rows : (n + 1) * rows]
    head_out = head_out.astype(BF16)
    group = heads * v_head
    mixed = jnp.zeros((rows, width), F32)
    for t in range(nx):
        piece = dot(head_out[:, t * group : (t + 1) * group], wo[t].reshape(group, width))
        mixed = mixed + piece.astype(BF16).astype(F32)
    residual = (toks + normalize(mixed, post_gain[...])).astype(BF16)
    ffn_in = normalize(residual, ffn_gain[...]).astype(BF16)

    gat[0] = ffn_in
    sent += ring_send(along_a, ring, lambda j: gat.at[0], gat, g_send, g_recv, far_first)
    ring_wait(along_a, ring, gw, gw_send, gw_recv, far_first)
    for i in range(ring):
        ws[0, i * rows : (i + 1) * rows, :] = gw[i]
    sent += ring_send(along_b, ring, lambda j: ws.at[0], ws, ws_send, ws_recv, far_first)
    take(len(back))
    ring_wait(along_a, ring, gat, g_send, g_recv, far_first)
    xs[0] = stack_rows(gat, stack_x, ring, rows)
    sent += ring_send(along_b, ring, lambda j: xs.at[0], xs, x_send, x_recv, far_first)
    early()
    block = ring * rows
    chip = (z * ny + y) * nc
    units = nc * dg.shape[1]
    dense_gate = dg[...].reshape(units, width)
    dense_up = du[...].reshape(units, width)
    dense_down = dd[...].reshape(units, width)
    down = wd[...].reshape(nc * wd.shape[2], width)
    for low, high in groups(ring):
        ring_wait(
            along_b, ring, xs, x_send, x_recv, [j for j in range(high - 1, low - 1, -1) if j]
        )
        count = (high - low) * block
        every = xs[low:high].reshape(count, width)
        spread = ws[low:high].reshape(count, experts)
        columns = lax.broadcasted_iota(jnp.int32, (count, experts), 1)
        acts = []
        for e in range(nc):
            share = jnp.sum(jnp.where(columns == chip + e, spread, 0.0), axis=1, keepdims=True)
            act = silu(dot(every, wg[e, 0])) * dot(every, wu[e, 0])
            acts.append((act * share).astype(BF16))
        gate = jnp.sum(every.astype(F32) * gate_vector[...], axis=1, keepdims=True)
        gate = 1.0 / (1.0 + jnp.exp(-gate))
        dense = silu(dot_nt(every, dense_gate)) * dot_nt(every, dense_up)
        dense = (dense * gate).astype(BF16)
        shares = dot(jnp.concatenate(acts, axis=1), down) + dot(dense, dense_down)
        outs[low:high] = shares.astype(BF16).reshape(high - low, block, width)
        sent += ring_send(
            along_b, ring, lambda j: outs.at[j], back_in, o_send, o_recv,
            [j for j in range(high - 1, low - 1, -1) if j],
        )
    if stop == 6:
        ring_wait(along_b, ring, back_in, o_send, o_recv, far_first)
        return finish()
    whole = outs[0].astype(F32)
    for j in far_first:
        ring_wait(along_b, ring, back_in, o_send, o_recv, [j])
        whole = whole + back_in[j].astype(F32)
    for i in range(ring):
        part_src[i] = whole[i * rows : (i + 1) * rows, :].astype(BF16)
    sent += ring_send(along_a, ring, lambda j: part_src.at[j], parts, p_send, p_recv, far_first)
    combined = part_src[0].astype(F32)
    for j in far_first:
        ring_wait(along_a, ring, parts, p_send, p_recv, [j])
        combined = combined + parts[j].astype(F32)
    output[...] = (residual.astype(F32) + normalize(combined, out_gain[...])).astype(BF16)
    for copy in sent:
        copy.wait_send()


def groups(ring):
    if ring == 8:
        return ((0, 1), (7, 8), (5, 7), (3, 5), (1, 3))
    return ((ring // 2, ring), (0, ring // 2))


def tail_kernel(a, b, c, a_out, b_out, c_out):
    a_out[...] = a[...]
    b_out[...] = b[...]
    c_out[...] = c[...]


def in_vmem(count):
    return [pl.BlockSpec(memory_space=pltpu.VMEM)] * count


def in_place(count):
    return [pl.BlockSpec(memory_space=pl.ANY)] * count


def semaphores(*counts):
    return [pltpu.SemaphoreType.DMA((n,)) for n in counts]


def shards(
    sizes,
    stop,
    tokens,
    lengths,
    cache_latent,
    cache_rope,
    attn_gain,
    latent_gain,
    post_gain,
    ffn_gain,
    out_gain,
    w_latent,
    w_rope_key,
    w_query,
    w_absorb_key,
    w_absorb_value,
    w_out,
    routes,
    route_weights,
    w_exp_gate,
    w_exp_up,
    w_exp_down,
    w_dense_gate,
    w_dense_up,
    w_dense_down,
    dense_gate_vector,
):
    rows, width = tokens.shape
    nz, ny, nc, nx = sizes["ep_0"], sizes["ep_1"], sizes["ep_2"], sizes["tp"]
    experts = nz * ny * nc
    heads, nope, rank = w_absorb_key.shape
    rope = w_rope_key.shape[1]
    part = w_latent.shape[1]
    floats = part + heads * rope
    inverse = np.float32(rope_base) ** (-np.arange(rope // 2, dtype=np.float32) / (rope // 2))
    inverse = np.concatenate([inverse, inverse])[None]
    V = pltpu.VMEM
    weights = (w_exp_gate, w_exp_up, w_exp_down, w_dense_gate, w_dense_up, w_dense_down)
    outs = (
        jax.ShapeDtypeStruct((rows, width), BF16),
        jax.ShapeDtypeStruct((rows, rank), BF16),
        jax.ShapeDtypeStruct((rows, rope), BF16),
    )
    args = (
        lengths, tokens, jnp.asarray(inverse), attn_gain[None], latent_gain[None], post_gain[None],
        ffn_gain[None], out_gain[None], dense_gate_vector[None], routes, route_weights,
        w_latent.T, w_rope_key.T, w_query.T, w_absorb_key, jnp.swapaxes(w_absorb_value, 1, 2),
        w_out.reshape(heads, -1, width), cache_latent, cache_rope, *weights,
    )
    results = pl.pallas_call(
        functools.partial(layer_kernel, sizes, stop),
        out_shape=tuple(V(o.shape, o.dtype) for o in outs),
        in_specs=in_place(len(args)),
        out_specs=tuple(in_vmem(3)),
        scratch_shapes=[
            pltpu.SMEM(lengths.shape, jnp.int32),
            V((rows, width), BF16),
            V((1, rope), F32),
            V((1, width), F32),
            V((1, rank), F32),
            V((1, width), F32),
            V((1, width), F32),
            V((1, width), F32),
            V((1, width), F32),
            V(routes.shape, jnp.int32),
            V(route_weights.shape, F32),
            V((heads * nope + floats, width), BF16),
            V((rope, width), BF16),
            V(w_absorb_key.shape, BF16),
            V((nx, heads, w_absorb_value.shape[2], rank), BF16),
            V((nx, heads, w_absorb_value.shape[2], width), BF16),
            V(cache_latent.shape, BF16),
            V(cache_rope.shape, BF16),
            *[V((nc, *w.shape), BF16) for w in weights],
            V((nx, rows, width), BF16),
            V((nx * rows, width), F32),
            V((nx, heads, rows, rank), BF16),
            V((nx, heads, rows, rank), BF16),
            V((nx, rows, floats), F32),
            V((nx, rows, floats), F32),
            V((heads * nope, heads * rank), BF16),
            V((nx * heads * rows, rank), F32),
            V((nx * heads * rows, rope), F32),
            V((nx * heads * rows, rank), F32),
            V((nx * heads * rows, rope), F32),
            V((ny, rows, experts), F32),
            V((ny, ny * rows, experts), F32),
            V((ny, rows, width), BF16),
            V((ny * rows, width), F32),
            V((ny, ny * rows, width), BF16),
            V((ny, ny * rows, width), BF16),
            V((ny, ny * rows, width), BF16),
            V((ny, rows, width), BF16),
            V((ny, rows, width), BF16),
        ]
        + [pltpu.SemaphoreType.REGULAR] * 2
        + semaphores(40, 6, 6, *([nx - 1, nx] * 3), *([nx - 1] * 8), *([ny] * 12)),
        compiler_params=pltpu.CompilerParams(collective_id=0, has_side_effects=True),
        name="layer",
    )(*args)
    return pl.pallas_call(
        tail_kernel,
        out_shape=outs,
        in_specs=in_vmem(3),
        out_specs=tuple(in_vmem(3)),
        name="tail",
    )(*[pltpu.with_memory_space_constraint(r, pltpu.VMEM) for r in results])


def solution(mesh, dims=(8, 8, 2), stop=0):
    torus = Mesh(mesh.devices.reshape(*dims, mesh.shape["tp"]), EP_TP)
    placed = (
        P(EP_TP, None),
        P(EP_TP),
        P(EP_TP, None, None),
        P(EP_TP, None, None),
        P(),
        P(),
        P(),
        P(),
        P(),
        P(None, "tp"),
        P(),
        P(None, "tp"),
        P("tp", None, None),
        P("tp", None, None),
        P("tp", None),
        P(EP_TP, None),
        P(EP_TP, None),
        P(EP, None, None),
        P(EP, None, None),
        P(EP, None, None),
        P(EP, None),
        P(EP, None),
        P(EP, None),
        P(),
    )
    return jax.shard_map(
        functools.partial(shards, dict(torus.shape), stop),
        mesh=torus,
        in_specs=placed,
        out_specs=(P(EP_TP, None), P(EP_TP, None), P(EP_TP, None)),
        check_vma=False,
    )
```
